32 devices in a mesh: gr: 2 (over x), sp: 8 (over z, y), tp: 2 (over core).
Axes of the slice: x: 2, y: 2, z: 4, core: 2. Of those that a mesh axis runs over, the one named last changes fastest.
Arguments:
- prompt_elements: bfloat16 [4, 2048, 2048], P('gr', 'sp'), may hold values from -6 to 6
- address_weights: bfloat16 [2048, 1024], P(None, 'tp'), may hold values from -0.125 to 0.125
- content_weights: bfloat16 [2048, 1024], P(None, 'tp'), may hold values from -0.125 to 0.125
- lookup_weights: bfloat16 [2048, 1024], P(None, 'tp'), may hold values from -0.125 to 0.125
- forgetting_weights: bfloat16 [2048, 8], replicated, may hold values from -0.125 to 0.125
- update_intensity_weights: bfloat16 [2048, 8], replicated, may hold values from -0.125 to 0.125
- forgetting_speeds: float32 [8], P('tp'), may hold values from 4.8828125e-05 to 0.05, as said below
- update_intensity_ceiling: float32 [8], P('tp'), may hold values from 0.03125 to 0.125, as said below
- forgetting_multiplier: float32 [4, 2048, 8], P('gr', 'sp', 'tp'), may hold values from 0.35 to 2.8, as said below
- spike_offsets: float32 [4, 2048, 8], P('gr', 'sp', 'tp'), may hold values from -0.7 to 0, as said below
- upcoming_element_vector: bfloat16 [4, 2048], P('gr'), may hold values from -6 to 6
- retrieval_rms_multiplier: float32 [128], replicated, may hold values from 0.1 to 1.9
Outputs:
- cache: bfloat16 [4, 8, 128, 128], P('gr', 'tp', 'sp')
- read: bfloat16 [4, 1024], P('gr', 'tp')
The draws below stay inside these ranges and needn't reach their ends.
Inputs may be any that keep to these rules, and one draw needn't show every extreme that they name: `forgetting_speeds`: per-head rates of decay. `update_intensity_ceiling`: per-head strength scales. `forgetting_multiplier`: positive factors. `spike_offsets`: non-positive log factors.
All inputs are finite; a program needn't handle non-finite values.
Results may differ from the reference program's by a relative error of at most 0.0037.
Values sent between devices are 32-bit elements; how exact they have to be, the bound alone decides.
No kernel may reach another device: no remote copies, remote signals or barrier semaphores. Data moves between devices by JAX's collectives and lax.ppermute only.
A program may use at most 64 MiB of HBM per device.

```python
import math
import jax
import jax.numpy as jnp
from jax import lax

D = 2048
H = 8
DK = 128
BLK = 64
SPAN = 256
NSEQ = 4
LEN = 2048


def draw_forgetting_speeds(key, part):
    order_key, level_key = jax.random.split(jax.random.fold_in(key, 17))
    ranks = jax.random.permutation(order_key, H)
    slow = ranks < H // 2
    level = jax.random.uniform(level_key, (H,), jnp.float32)
    slow_rate = (0.1 + 0.4 * level) / LEN
    fast_rate = 0.02 + 0.03 * level
    return jnp.where(slow, slow_rate, fast_rate).astype(jnp.float32)


def draw_update_intensity_ceiling(key, part):
    level = jax.random.uniform(jax.random.fold_in(key, 19), (H,), jnp.float32, math.log(0.5), math.log(2.0))
    return (jnp.exp(level) * DK / LEN).astype(jnp.float32)


def draw_forgetting_multiplier(key, part):
    bottom, top = (0.5, 2.0)
    level = jax.random.uniform(jax.random.fold_in(key, 23), (NSEQ, LEN // SPAN, H), jnp.float32, math.log(bottom), math.log(top))
    return jnp.repeat(jnp.exp(level), SPAN, axis=1).astype(jnp.float32)


def draw_spike_offsets(key, part):
    hit_key, depth_key = jax.random.split(jax.random.fold_in(key, 29))
    hits = jax.random.uniform(hit_key, (NSEQ, LEN, H), jnp.float32) < 4.0 / LEN
    depth = jax.random.uniform(depth_key, (NSEQ, LEN, H), jnp.float32, math.log(0.5), math.log(0.8))
    return jnp.where(hits, depth, 0.0).astype(jnp.float32)


def level_of(stream_key, extent, cuts, smallest, high):
    gain = 1.0
    for position, blocks in cuts:
        heights = jax.random.uniform(jax.random.fold_in(jax.random.fold_in(stream_key, 6), position), (blocks,), jnp.float32, smallest / len(cuts), high / len(cuts))
        gain = gain * jnp.repeat(jnp.exp(heights), extent[position] // blocks).reshape((-1,) + (1,) * (len(extent) - 1 - position))
    return gain


def bell_draw(own_key, extent, scale, bound, cuts=(), held_as=jnp.bfloat16):
    values = jax.random.normal(own_key, extent, jnp.float32) * scale
    if len(cuts) > 0:
        values = level_of(own_key, extent, cuts, -0.22, 0.18) * values
    return jnp.clip(values, min=-bound, max=bound).astype(held_as)


def setup_inputs(seed: int = 0) -> dict:
    key_list = jax.random.split(jax.random.key(seed), 13)
    prompt_elements = bell_draw(key_list[0], (NSEQ, LEN, D), 1.0, 6.0, ((0, 2), (1, 8)))
    address_weights = bell_draw(key_list[1], (D, H * DK), D ** -0.5, 0.125, ((1, 2),))
    content_weights = bell_draw(key_list[2], (D, H * DK), D ** -0.5, 0.125, ((1, 2),))
    lookup_weights = bell_draw(key_list[3], (D, H * DK), D ** -0.5, 0.125, ((1, 2),))
    forgetting_weights = bell_draw(key_list[4], (D, H), D ** -0.5, 0.125)
    update_intensity_weights = bell_draw(key_list[5], (D, H), D ** -0.5, 0.125)
    forgetting_speeds = draw_forgetting_speeds(jax.random.fold_in(key_list[12], 71), 0)
    update_intensity_ceiling = draw_update_intensity_ceiling(jax.random.fold_in(key_list[12], 71), 0)
    forgetting_multiplier = draw_forgetting_multiplier(jax.random.fold_in(key_list[12], 71), 0)
    spike_offsets = draw_spike_offsets(jax.random.fold_in(key_list[12], 71), 0)
    upcoming_element_vector = bell_draw(key_list[10], (NSEQ, D), 1.0, 6.0, ((0, 2),))
    retrieval_rms_multiplier = jnp.clip(1.0 + 0.18 * jax.random.normal(key_list[11], (DK,), jnp.float32), 0.1, 1.9)
    return dict(prompt_elements=prompt_elements, address_weights=address_weights, content_weights=content_weights, lookup_weights=lookup_weights, forgetting_weights=forgetting_weights, update_intensity_weights=update_intensity_weights, forgetting_speeds=forgetting_speeds, update_intensity_ceiling=update_intensity_ceiling, forgetting_multiplier=forgetting_multiplier, spike_offsets=spike_offsets, upcoming_element_vector=upcoming_element_vector, retrieval_rms_multiplier=retrieval_rms_multiplier)


HIGH = lax.Precision.HIGHEST
EPS = 1e-06

def silu_f(values):
    return values * jax.nn.sigmoid(values)

def unit_rows(values):
    return values * lax.rsqrt(lax.optimization_barrier(jnp.sum(values * values, axis=-1, keepdims=True)) + EPS)

def unit_inverse(lower):
    eye = jnp.eye(lower.shape[-1], dtype=jnp.float32)
    power = -lower
    result = eye + power
    degree = 2
    while degree < lower.shape[-1]:
        power = jnp.matmul(power, power, precision=HIGH)
        result = jnp.matmul(result, eye + power, precision=HIGH)
        degree = degree * 2
    return result

def head_inputs(flat, address_weights, content_weights, decay_cols, strength_cols, forgetting_speeds, update_intensity_ceiling, head_dim):
    count = flat.shape[0]
    key_raw = lax.optimization_barrier(jnp.dot(flat, address_weights, preferred_element_type=jnp.float32).astype(jnp.bfloat16))
    value_raw = lax.optimization_barrier(jnp.dot(flat, content_weights, preferred_element_type=jnp.float32).astype(jnp.bfloat16))
    keys = unit_rows(silu_f(key_raw.astype(jnp.float32)).reshape(count, -1, head_dim))
    values = silu_f(value_raw.astype(jnp.float32)).reshape(count, -1, head_dim)
    decay_pre = jnp.dot(flat, decay_cols, preferred_element_type=jnp.float32)
    strength_pre = jnp.dot(flat, strength_cols, preferred_element_type=jnp.float32)
    speed_addend = -forgetting_speeds * jax.nn.softplus(decay_pre)
    strength = update_intensity_ceiling * jax.nn.sigmoid(strength_pre)
    return (keys, values, speed_addend, strength)

def to_blocks(values, seqs):
    shaped = values.reshape((seqs, -1) + values.shape[1:])
    moved = jnp.moveaxis(shaped, 2, 1)
    return moved.reshape((moved.shape[0] * moved.shape[1], -1, BLK) + moved.shape[3:])

def block_terms(keys, values, forgetting_exponent, strength):
    size = keys.shape[2]
    cumulative = jnp.cumsum(forgetting_exponent, axis=-1)
    places = jnp.arange(size)
    inclusive = places[:, None] >= places[None, :]
    strict = places[:, None] > places[None, :]
    spread = jnp.where(inclusive, cumulative[..., :, None] - cumulative[..., None, :], -jnp.inf)
    weighted = keys * strength[..., None]
    lower = jnp.where(strict, jnp.einsum('gncd,gnmd->gncm', weighted, keys, precision=HIGH) * jnp.exp(spread), 0.0)
    solved = unit_inverse(lower)
    targets = jnp.matmul(solved, values * strength[..., None], precision=HIGH)
    erasers = jnp.matmul(solved, weighted * jnp.exp(cumulative)[..., None], precision=HIGH)
    final_log = cumulative[..., -1]
    faded = keys * jnp.exp(final_log[..., None] - cumulative)[..., None]
    return (targets, erasers, faded, final_log)

def finish(query, keys, values, speed_addend, strength, query_state, key_state, retrieval_rms_multiplier):
    match = lax.optimization_barrier(jnp.sum(query * keys, axis=-1)) * strength
    fading = jnp.exp(speed_addend)
    mixed = fading[..., None] * (query_state - match[..., None] * key_state) + match[..., None] * values
    scaled = mixed * lax.rsqrt(lax.optimization_barrier(jnp.mean(mixed * mixed, axis=-1, keepdims=True)) + EPS) * retrieval_rms_multiplier
    return scaled.reshape(scaled.shape[0], -1).astype(jnp.bfloat16)

def new_query(upcoming_element_vector, lookup_weights, head_dim):
    query_raw = lax.optimization_barrier(jnp.dot(upcoming_element_vector, lookup_weights, preferred_element_type=jnp.float32).astype(jnp.bfloat16))
    query = unit_rows(silu_f(query_raw.astype(jnp.float32)).reshape(upcoming_element_vector.shape[0], -1, head_dim))
    return query * head_dim ** (-0.5)

def reference(prompt_elements, address_weights, content_weights, lookup_weights, forgetting_weights, update_intensity_weights, forgetting_speeds, update_intensity_ceiling, forgetting_multiplier, spike_offsets, upcoming_element_vector, retrieval_rms_multiplier):
    nseq, length, width = prompt_elements.shape
    head_dim = retrieval_rms_multiplier.shape[0]
    attention_group_number = forgetting_speeds.shape[0]
    flat = prompt_elements.reshape(nseq * length, width)
    keys, values, speed_addend, strength = head_inputs(flat, address_weights, content_weights, forgetting_weights, update_intensity_weights, forgetting_speeds, update_intensity_ceiling, head_dim)
    forgetting_exponent = speed_addend * forgetting_multiplier.reshape(-1, attention_group_number) + spike_offsets.reshape(-1, attention_group_number)
    targets, erasers, faded, final_log = block_terms(to_blocks(keys, nseq), to_blocks(values, nseq), to_blocks(forgetting_exponent, nseq), to_blocks(strength, nseq))

    def advance(state, inputs):
        target, eraser, fade, final = inputs
        fresh = target - jnp.matmul(eraser, state, precision=HIGH)
        state = state * jnp.exp(final)[:, None, None] + jnp.matmul(jnp.swapaxes(fade, -1, -2), fresh, precision=HIGH)
        return (state, None)
    moved = tuple((jnp.moveaxis(item, 1, 0) for item in (targets, erasers, faded, final_log)))
    state, _ = lax.scan(advance, jnp.zeros((nseq * attention_group_number, head_dim, head_dim), jnp.float32), moved)
    stored = state.reshape(nseq, attention_group_number, head_dim, head_dim)
    cache = stored.astype(jnp.bfloat16)
    query = new_query(upcoming_element_vector, lookup_weights, head_dim)
    new_keys, new_values, rate_new, strength_new = head_inputs(upcoming_element_vector, address_weights, content_weights, forgetting_weights, update_intensity_weights, forgetting_speeds, update_intensity_ceiling, head_dim)
    query_state = jnp.einsum('shk,shkv->shv', query, stored, precision=HIGH)
    key_state = jnp.einsum('shk,shkv->shv', new_keys, stored, precision=HIGH)
    read = finish(query, new_keys, new_values, rate_new, strength_new, query_state, key_state, retrieval_rms_multiplier)
    return (cache, read)
```

```python
import jax
import jax.numpy as jnp
from jax import lax
from jax.experimental import pallas as pl
from jax.experimental.pallas import tpu as pltpu
from jax.sharding import PartitionSpec as P

EPS = 1e-06
CHUNK = 128
PAD = 8
F32 = jnp.float32
BF16 = jnp.bfloat16
WHOLE = pl.BlockSpec(memory_space=pltpu.VMEM)
SCALARS = pl.BlockSpec(memory_space=pltpu.SMEM)


def dot(a, b):
    return jnp.dot(a, b, preferred_element_type=F32)


def dot_nt(a, b):
    return lax.dot_general(a, b, (((1,), (1,)), ((), ())), preferred_element_type=F32)


def dot_tn(a, b):
    return lax.dot_general(a, b, (((0,), (0,)), ((), ())), preferred_element_type=F32)


def halves(a):
    high = a.astype(BF16)
    return high, (a - high.astype(F32)).astype(BF16)


def dot3(a, b):
    ah, al = halves(a)
    bh, bl = halves(b)
    return dot(ah, bh) + dot(ah, bl) + dot(al, bh)


def silu(values):
    return values * jax.nn.sigmoid(values)


def unit(values):
    return values * lax.rsqrt(jnp.sum(values * values, axis=-1, keepdims=True) + EPS)


def softplus(values):
    return jnp.maximum(values, 0.0) + jnp.log1p(jnp.exp(-jnp.abs(values)))


def pick_lane(values, lane):
    places = lax.broadcasted_iota(jnp.int32, values.shape, 1)
    return jnp.sum(jnp.where(places == lane, values, 0.0), axis=1, keepdims=True)


def chunk_terms(keys, values, strength, cumulative, cumulative_row):
    size = keys.shape[0]
    row = lax.broadcasted_iota(jnp.int32, (size, size), 0)
    col = lax.broadcasted_iota(jnp.int32, (size, size), 1)
    strict = row > col
    short = keys.astype(BF16)
    gram = dot_nt(short, short)
    spread = jnp.exp(jnp.minimum(cumulative - cumulative_row, 0.0))
    lower = jnp.where(strict, gram * strength * spread, 0.0)

    def level(m):
        return (row // (2 * m) == col // (2 * m)) & (row // m != col // m)

    inverse = jnp.where(row == col, 1.0, 0.0) - jnp.where(level(1), lower, 0.0)
    m = 2
    while m < size:
        block = jnp.where(level(m), lower, 0.0).astype(BF16)
        held = inverse.astype(BF16)
        if m < 16:
            inverse = inverse - dot(dot(held, block).astype(BF16), held)
        else:
            odd = [slice(i, i + m) for i in range(m, size, 2 * m)]
            picked = jnp.concatenate([held[s] for s in odd], axis=0)
            change = dot(dot(picked, block).astype(BF16), held)
            parts = []
            for i in range(len(odd)):
                parts.append(inverse[i * 2 * m : i * 2 * m + m])
                parts.append(inverse[odd[i]] - change[i * m : i * m + m])
            inverse = jnp.concatenate(parts, axis=0)
        m *= 2
    off = jnp.where(strict, inverse, 0.0).astype(BF16)
    grown = jnp.exp(cumulative)
    source = jnp.concatenate([keys * (strength * grown), values * strength], axis=1)
    solved = source + dot(off, source.astype(BF16))
    last = cumulative[size - 1 : size]
    faded = (keys * jnp.exp(last - cumulative)).astype(BF16)
    both = dot_tn(faded, solved.astype(BF16))
    width = keys.shape[1]
    return both[:, :width], both[:, width:], jnp.exp(last)


def local_maps_kernel(
    x_ref, wk_ref, wv_ref, wd_ref, ws_ref, speed_ref, ceil_ref, mult_ref, spike_ref,
    keep_ref, send_ref, beta_s, cum_s, row_s,
):
    head = pl.program_id(0)
    seqs, span, width = x_ref.shape
    heads = speed_ref.shape[1]
    dim = wk_ref.shape[1]
    count = seqs * span
    chunks = count // CHUNK
    flat = x_ref[...].reshape(count, width)

    @pl.when(head == 0)
    def _():
        shard = lax.axis_index("tp")

        def mine(full):
            part = full[:, :heads]
            for t in range(1, full.shape[1] // heads):
                part = jnp.where(shard == t, full[:, t * heads : (t + 1) * heads], part)
            return part

        decay_pre = mine(dot(flat, wd_ref[...]))
        strength_pre = mine(dot(flat, ws_ref[...]))
        rate = -speed_ref[...] * softplus(decay_pre)
        gates = rate * mult_ref[...].reshape(count, heads) + spike_ref[...].reshape(count, heads)
        beta_s[:, :heads] = ceil_ref[...] * jax.nn.sigmoid(strength_pre)
        row = lax.broadcasted_iota(jnp.int32, (CHUNK, CHUNK), 0)
        col = lax.broadcasted_iota(jnp.int32, (CHUNK, CHUNK), 1)
        ones = jnp.where(row >= col, 1.0, 0.0)
        for c in range(chunks):
            rows = slice(c * CHUNK, (c + 1) * CHUNK)
            cum_s[rows, :heads] = jnp.dot(
                ones, gates[rows], precision=lax.Precision.HIGHEST, preferred_element_type=F32
            )
            row_s[c] = cum_s[rows, :].T

    weights = jnp.concatenate([wk_ref[...], wv_ref[...]], axis=1)
    raw = dot(flat, weights).astype(BF16).astype(F32)
    keys = unit(silu(raw[:, :dim]))
    values = silu(raw[:, dim:])
    strength = pick_lane(beta_s[...], head)
    cumulative = pick_lane(cum_s[...], head)
    terms = []
    for c in range(chunks):
        rows = slice(c * CHUNK, (c + 1) * CHUNK)
        terms.append(
            chunk_terms(
                keys[rows], values[rows], strength[rows], cumulative[rows],
                row_s[c, pl.ds(head, 1), :],
            )
        )
    row = lax.broadcasted_iota(jnp.int32, (dim, dim), 0)
    col = lax.broadcasted_iota(jnp.int32, (dim, dim), 1)
    eye = jnp.where(row == col, 1.0, 0.0)
    maps = []
    for s in range(seqs):
        mine = terms[s * (chunks // seqs) : (s + 1) * (chunks // seqs)]
        eraser, target, decay = mine[0]
        held_a, held_b = decay * eye - eraser, target
        for eraser, target, decay in mine[1:]:
            both = dot(eraser.astype(BF16), jnp.concatenate([held_a, held_b], axis=1).astype(BF16))
            held_a = decay * held_a - both[:, :dim]
            held_b = decay * held_b - both[:, dim:] + target
        maps.append((held_a, held_b))
    bit = lax.axis_index("sp") % 2
    half = seqs // 2
    for s in range(half):
        for part in range(2):
            first, second = maps[s][part], maps[s + half][part]
            rows = slice(part * dim, (part + 1) * dim)
            keep_ref[s, 0, rows, :] = jnp.where(bit == 0, first, second)
            send_ref[s, 0, rows, :] = jnp.where(bit == 0, second, first)


def local_maps(x, wk, wv, wd, ws, speeds, ceilings, mult, spikes, dim):
    seqs, span, width = x.shape
    heads = speeds.shape[0]
    count = seqs * span
    constant = lambda *shape: pl.BlockSpec(shape, lambda h: (0,) * len(shape))
    column = pl.BlockSpec((width, dim), lambda h: (0, h))
    result = jax.ShapeDtypeStruct((seqs // 2, heads, 2 * dim, dim), F32)
    place = pl.BlockSpec((seqs // 2, 1, 2 * dim, dim), lambda h: (0, h, 0, 0))
    return pl.pallas_call(
        local_maps_kernel,
        grid=(heads,),
        in_specs=[
            constant(*x.shape), column, column, constant(*wd.shape), constant(*ws.shape),
            constant(1, heads), constant(1, heads), constant(*mult.shape), constant(*spikes.shape),
        ],
        out_specs=[place, place],
        out_shape=[result, result],
        scratch_shapes=[
            pltpu.VMEM((count, 128), F32),
            pltpu.VMEM((count, 128), F32),
            pltpu.VMEM((count // CHUNK, 128, 128), F32),
        ],
        name="local_maps",
    )(x, wk, wv, wd, ws, speeds.reshape(1, -1), ceilings.reshape(1, -1), mult, spikes)


def new_token_kernel(
    x_ref, wk_ref, wv_ref, wq_ref, wd_ref, ws_ref, speed_ref, ceil_ref, out_ref
):
    head = pl.program_id(0)
    dim = wk_ref.shape[1]
    x = x_ref[...]
    lane = lax.axis_index("tp") * speed_ref.shape[0] + head

    def project(w_ref):
        return dot(x, w_ref[...]).astype(BF16).astype(F32)

    query = unit(silu(project(wq_ref))) * dim ** (-0.5)
    keys = unit(silu(project(wk_ref)))
    values = silu(project(wv_ref))
    decay_pre = pick_lane(dot(x, wd_ref[...]), lane)
    strength_pre = pick_lane(dot(x, ws_ref[...]), lane)
    fading = jnp.exp(-speed_ref[head] * softplus(decay_pre))
    match = jnp.sum(query * keys, axis=-1, keepdims=True) * (
        ceil_ref[head] * jax.nn.sigmoid(strength_pre)
    )
    items = [query, keys, values, jnp.broadcast_to(fading, query.shape), jnp.broadcast_to(match, query.shape)]
    for s in range(x.shape[0]):
        for i, item in enumerate(items):
            out_ref[s, 0, i : i + 1, :] = item[s : s + 1]


def new_token(x, wk, wv, wq, wd, ws, speeds, ceilings, dim):
    seqs, width = x.shape
    heads = speeds.shape[0]
    constant = lambda *shape: pl.BlockSpec(shape, lambda h: (0,) * len(shape))
    column = pl.BlockSpec((width, dim), lambda h: (0, h))
    return pl.pallas_call(
        new_token_kernel,
        grid=(heads,),
        in_specs=[
            constant(*x.shape), column, column, column, constant(*wd.shape), constant(*ws.shape),
            SCALARS, SCALARS,
        ],
        out_specs=pl.BlockSpec((seqs, 1, PAD, dim), lambda h: (0, h, 0, 0)),
        out_shape=jax.ShapeDtypeStruct((seqs, heads, PAD, dim), F32),
        name="new_token",
    )(x, wk, wv, wq, wd, ws, speeds, ceilings)


def joined(keep, got, bit, dim):
    early = jnp.where(bit == 0, keep, got)
    late = jnp.where(bit == 0, got, keep)
    early = jnp.concatenate([early[:dim], early[dim:]], axis=1)
    both = dot3(late[:dim], early)
    return both[:, :dim], both[:, dim:] + late[dim:]


def join_kernel(keep_ref, got_ref, *outs, stage, split):
    states, rows, dim = keep_ref.shape
    place = lax.axis_index("sp")
    bit = (place >> stage) % 2
    half = states // 2 if split else states
    following = (place >> (stage + 1)) % 2
    for which, out in enumerate(outs):
        for i in range(half):
            at = i + half * (following ^ which) if split else i
            out_a, out_b = joined(keep_ref[at], got_ref[at], bit, dim)
            out[i, :dim, :] = out_a
            out[i, dim:, :] = out_b


def join(keep, got, stage, split):
    states, rows, dim = keep.shape
    count = states // 2 if split else states
    shape = jax.ShapeDtypeStruct((count, rows, dim), F32)
    return pl.pallas_call(
        lambda *refs: join_kernel(*refs, stage=stage, split=split),
        in_specs=[WHOLE, WHOLE],
        out_specs=[WHOLE] * (2 if split else 1),
        out_shape=[shape] * (2 if split else 1),
        name="join",
    )(keep, got)


def state_of(index, place, seqs, heads, split_bits):
    states = seqs * heads
    base = 0
    for b in range(split_bits):
        states //= 2
        base = base + ((place >> b) % 2) * states
    at = base + index
    return at // heads, at % heads


def pack_kernel(keep_ref, got_ref, token_ref, own_ref, send_ref, *, stage, split_bits):
    states, rows, dim = keep_ref.shape
    seqs, heads = token_ref.shape[:2]
    place = lax.axis_index("sp")
    bit = (place >> stage) % 2
    right = (place >> (stage + 1)) % 2 == 1
    half = dim // 2
    for i in range(states):
        s, h = state_of(i, place, seqs, heads, split_bits)
        out_a, out_b = joined(keep_ref[i], got_ref[i], bit, dim)
        token = token_ref[s, h][:2]
        reads = dot3(jnp.concatenate([token, token, token, token], axis=0), jnp.concatenate([out_a, out_b], axis=1))
        tail = jnp.concatenate([reads[:2, :dim], reads[:2, dim:], reads[:4, :dim]], axis=0)
        own_ref[i, :half, :] = jnp.where(right, out_a[half:], out_b[:half])
        own_ref[i, half:dim, :] = jnp.where(right, out_b[half:], out_b[half:])
        own_ref[i, dim:, :] = tail
        send_ref[i, :half, :] = jnp.where(right, out_a[:half], out_b[:half])
        send_ref[i, half:dim, :] = jnp.where(right, out_b[:half], out_b[half:])
        send_ref[i, dim:, :] = tail


def pack(keep, got, token, stage, split_bits):
    states, rows, dim = keep.shape
    shape = jax.ShapeDtypeStruct((states, dim + PAD, dim), F32)
    return pl.pallas_call(
        lambda *refs: pack_kernel(*refs, stage=stage, split_bits=split_bits),
        in_specs=[WHOLE] * 3,
        out_specs=[WHOLE] * 2,
        out_shape=[shape] * 2,
        name="pack",
    )(keep, got, token)


def finish_kernel(own_ref, got_ref, token_ref, gain_ref, *rest, stage, split_bits, block):
    outs, rows_s = rest[:-1], rest[-1]
    states, _, dim = own_ref.shape
    seqs, heads = token_ref.shape[:2]
    place = lax.axis_index("sp")
    right = (place >> stage) % 2 == 1
    half = dim // 2
    reads = []
    for i in range(states):
        s, h = state_of(i, place, seqs, heads, split_bits)
        own, got = own_ref[i], got_ref[i]
        state = jnp.where(right, got[:dim], own[:dim])
        later = jnp.where(right, own, got)
        full = dot3(jnp.concatenate([later[:half], later[dim:]], axis=0), state)
        rows_s[i] = full[:half] + later[half:dim]
        seen = full[half : half + 2] + later[dim + 2 : dim + 4]
        token = token_ref[s, h]
        fading, match = token[3:4], token[4:5]
        mixed = fading * (seen[:1] - match * seen[1:2]) + match * token[2:3]
        scale = lax.rsqrt(jnp.mean(mixed * mixed, axis=-1, keepdims=True) + EPS)
        reads.append(mixed * scale * gain_ref[...])
    blocks = half // block
    for mask, out in enumerate(outs):
        start = ((place ^ mask) % blocks) * block
        for i in range(states):
            out[i * block : (i + 1) * block, :] = rows_s[i, pl.ds(start, block), :]
            out[states * block + i : states * block + i + 1, :] = reads[i]


def finish(own, got, token, gain, stage, split_bits, block):
    states, _, dim = own.shape
    rows = -(-(states * block + states) // PAD) * PAD
    shape = jax.ShapeDtypeStruct((rows, dim), F32)
    count = 2**split_bits
    return pl.pallas_call(
        lambda *refs: finish_kernel(
            *refs, stage=stage, split_bits=split_bits, block=block
        ),
        in_specs=[WHOLE] * 4,
        out_specs=[WHOLE] * count,
        out_shape=[shape] * count,
        scratch_shapes=[pltpu.VMEM((states, dim // 2, dim), F32)],
        name="finish",
    )(own, got, token, gain.reshape(1, -1))


def place_kernel(*refs, count, split_bits, block):
    ins, cache_ref, read_ref, reads_s = refs[:count], refs[count], refs[count + 1], refs[count + 2]
    seqs, heads, _, dim = cache_ref.shape
    states = seqs * heads // count
    place = lax.axis_index("sp")
    for mask, got in enumerate(ins):
        for i in range(states):
            s, h = state_of(i, place ^ mask, seqs, heads, split_bits)
            cache_ref[s, h] = got[i * block : (i + 1) * block, :].astype(BF16)
            reads_s[pl.ds(s * heads + h, 1), :] = got[states * block + i : states * block + i + 1, :]
    for h in range(heads):
        rows = [reads_s[s * heads + h : s * heads + h + 1, :] for s in range(seqs)]
        read_ref[:, h * dim : (h + 1) * dim] = jnp.concatenate(rows, axis=0).astype(BF16)


def place_outputs(parts, seqs, heads, dim, block, split_bits):
    count = len(parts)
    return pl.pallas_call(
        lambda *refs: place_kernel(*refs, count=count, split_bits=split_bits, block=block),
        in_specs=[WHOLE] * count,
        out_specs=[WHOLE] * 2,
        out_shape=[
            jax.ShapeDtypeStruct((seqs, heads, block, dim), BF16),
            jax.ShapeDtypeStruct((seqs, heads * dim), BF16),
        ],
        scratch_shapes=[pltpu.VMEM((seqs * heads, dim), F32)],
        name="place_outputs",
    )(*parts)


def on_device(
    prompt_elements, address_weights, content_weights, lookup_weights, forgetting_weights,
    update_intensity_weights, forgetting_speeds, update_intensity_ceiling, forgetting_multiplier,
    spike_offsets, upcoming_element_vector, retrieval_rms_multiplier,
):
    seqs = prompt_elements.shape[0]
    dim = retrieval_rms_multiplier.shape[0]
    heads = forgetting_speeds.shape[0]
    places = lax.axis_size("sp")
    stages = places.bit_length() - 1
    block = dim // places

    def exchange(values, mask):
        return lax.ppermute(values, "sp", [(i, i ^ mask) for i in range(places)])

    keep, send = local_maps(
        prompt_elements, address_weights, content_weights, forgetting_weights,
        update_intensity_weights, forgetting_speeds, update_intensity_ceiling,
        forgetting_multiplier, spike_offsets, dim,
    )
    states = seqs * heads // 2
    keep = keep.reshape(states, 2 * dim, dim)
    got = exchange(send.reshape(states, 2 * dim, dim), 1)
    token = new_token(
        upcoming_element_vector, address_weights, content_weights, lookup_weights,
        forgetting_weights, update_intensity_weights, forgetting_speeds,
        update_intensity_ceiling, dim,
    )
    split_bits = 1
    for stage in range(stages - 2):
        split = states % 2 == 0 and split_bits == stage + 1
        if split:
            keep, send = join(keep, got, stage, True)
            states //= 2
            split_bits += 1
        else:
            (keep,) = join(keep, got, stage, False)
            send = keep
        got = exchange(send, 2 ** (stage + 1))
    own, send = pack(keep, got, token, stages - 2, split_bits)
    got = exchange(send, 2 ** (stages - 1))
    parts = finish(own, got, token, retrieval_rms_multiplier, stages - 1, split_bits, block)
    parts = [part if mask == 0 else exchange(part, mask) for mask, part in enumerate(parts)]
    cache, read = place_outputs(parts, seqs, heads, dim, block, split_bits)
    return cache, read


def solution(mesh):
    in_specs = (
        P("gr", "sp", None),
        P(None, "tp"),
        P(None, "tp"),
        P(None, "tp"),
        P(),
        P(),
        P("tp"),
        P("tp"),
        P("gr", "sp", "tp"),
        P("gr", "sp", "tp"),
        P("gr", None),
        P(),
    )
    out_specs = (P("gr", "tp", "sp", None), P("gr", "tp"))
    return jax.shard_map(
        on_device, mesh=mesh, in_specs=in_specs, out_specs=out_specs, check_vma=False
    )
```

```python
import jax
import jax.numpy as jnp
from jax import lax
from jax.experimental import pallas as pl
from jax.experimental.pallas import tpu as pltpu
from jax.sharding import PartitionSpec as P

EPS = 1e-06
CHUNK = 128
PAD = 8
F32 = jnp.float32
BF16 = jnp.bfloat16
WHOLE = pl.BlockSpec(memory_space=pltpu.VMEM)
LIMIT = pltpu.CompilerParams(vmem_limit_bytes=16 * 2**20)


def dot(a, b):
    return jnp.dot(a, b, preferred_element_type=F32)


def dot_nt(a, b):
    return lax.dot_general(a, b, (((1,), (1,)), ((), ())), preferred_element_type=F32)


def dot_tn(a, b):
    return lax.dot_general(a, b, (((0,), (0,)), ((), ())), preferred_element_type=F32)


def halves(a):
    high = a.astype(BF16)
    return high, (a - high.astype(F32)).astype(BF16)


def dot3(a, b):
    ah, al = halves(a)
    bh, bl = halves(b)
    return dot(ah, bh) + dot(ah, bl) + dot(al, bh)


def silu(values):
    return values * jax.nn.sigmoid(values)


def unit(values):
    return values * lax.rsqrt(jnp.sum(values * values, axis=-1, keepdims=True) + EPS)


def softplus(values):
    return jnp.maximum(values, 0.0) + jnp.log1p(jnp.exp(-jnp.abs(values)))


def pick_lane(values, lane):
    places = lax.broadcasted_iota(jnp.int32, values.shape, 1)
    return jnp.sum(jnp.where(places == lane, values, 0.0), axis=1, keepdims=True)


def gate_tables(x, wd, ws, speeds, ceilings, mult, spike, heads, upper):
    total = wd.shape[0]
    rates = jnp.concatenate([wd.astype(F32), ws.astype(F32)], axis=0)
    both = dot_nt(rates.astype(BF16), x)
    shard = lax.axis_index("tp")
    row = lax.broadcasted_iota(jnp.int32, (heads, heads), 0)
    col = lax.broadcasted_iota(jnp.int32, (heads, heads), 1)

    def mine(full):
        part = full[:heads]
        for t in range(1, total // heads):
            part = jnp.where(shard == t, full[t * heads : (t + 1) * heads], part)
        return part

    def upright(values):
        return jnp.sum(jnp.where(row == col, values[:, :heads], 0.0), axis=1, keepdims=True)

    gates = -upright(speeds) * softplus(mine(both[:total])) * mult + spike
    beta = upright(ceilings) * jax.nn.sigmoid(mine(both[total:]))
    rows = []
    for c in range(x.shape[0] // CHUNK):
        lanes = slice(c * CHUNK, (c + 1) * CHUNK)
        rows.append(beta[:, lanes])
        rows.append(
            jnp.dot(gates[:, lanes], upper, precision=lax.Precision.HIGHEST, preferred_element_type=F32)
        )
    fill = -sum(r.shape[0] for r in rows) % PAD
    if fill:
        rows.append(jnp.zeros((fill, CHUNK), F32))
    return jnp.concatenate(rows, axis=0)


def local_maps_kernel(*refs, heads, own_heads, first):
    if first:
        x_hbm, wk_hbm, wv_hbm = refs[:3]
        small_hbm = refs[3:9]
        keep_ref, send_ref, table_ref = refs[9:12]
        k_s, v_s, lower_s, inverse_s, half_s, mask_s, x_s, w_s = refs[12:20]
        small_s = refs[20:26]
        sems = refs[26]
    else:
        x_s, wk_ref, wv_ref, table_ref = refs[:4]
        keep_ref, send_ref = refs[4:6]
        k_s, v_s, lower_s, inverse_s, half_s, mask_s = refs[6:12]
    seqs, span, width = x_s.shape
    dim = k_s.shape[-1]
    count = seqs * span
    chunks = count // CHUNK
    group = len(own_heads)
    steps = [2**i for i in range(CHUNK.bit_length() - 1)]

    if first:
        copies = [pltpu.make_async_copy(x_hbm.at[s], x_s.at[s], sems.at[s]) for s in range(seqs)]
        for i, (source, target) in enumerate(zip(small_hbm, small_s)):
            copies.append(pltpu.make_async_copy(source, target, sems.at[seqs + i]))
        base = len(copies)
        for g, h in enumerate(own_heads):
            for i, w_hbm in enumerate((wk_hbm, wv_hbm)):
                copies.append(
                    pltpu.make_async_copy(
                        w_hbm.at[:, pl.ds(h * dim, dim)],
                        w_s.at[g, :, pl.ds(i * dim, dim)],
                        sems.at[base + 2 * g + i],
                    )
                )
        for copy in copies:
            copy.start()

    row = lax.broadcasted_iota(jnp.int32, (CHUNK, CHUNK), 0)
    col = lax.broadcasted_iota(jnp.int32, (CHUNK, CHUNK), 1)
    strict = row > col
    eye = jnp.where(row == col, 1.0, 0.0)

    def level(m):
        return (row // (2 * m) == col // (2 * m)) & (row // m != col // m)

    for i, m in enumerate(steps):
        mask_s[i] = jnp.where(level(m), 1.0, 0.0).astype(BF16)
    mask_s[len(steps)] = jnp.where(strict, 1.0, 0.0).astype(BF16)

    if first:
        for copy in copies[:base]:
            copy.wait()
    flat = x_s[...].reshape(count, width)
    if first:
        wd, ws, speeds, ceilings = (ref[...] for ref in small_s[:4])
        mult, spike = (
            jnp.concatenate([ref[s] for s in range(seqs)], axis=1) for ref in small_s[4:]
        )
        table_ref[...] = gate_tables(
            flat, wd, ws, speeds, ceilings, mult, spike, heads, jnp.where(row <= col, 1.0, 0.0)
        )
    columns = table_ref[...].T

    def at(c, g, which):
        return (2 * c + which) * heads + own_heads[g]

    def column(c, g, which):
        return jnp.broadcast_to(columns[:, at(c, g, which) : at(c, g, which) + 1], (CHUNK, CHUNK))

    pieces = [(g, c) for g in range(group) for c in range(chunks)]

    for g, h in enumerate(own_heads):
        if first:
            copies[base + 2 * g].wait()
            copies[base + 2 * g + 1].wait()
            weights = w_s[g]
        else:
            lanes = slice(h * dim, (h + 1) * dim)
            weights = jnp.concatenate([wk_ref[:, lanes], wv_ref[:, lanes]], axis=1)
        raw = dot(flat, weights).astype(BF16).astype(F32)
        k_s[g] = unit(silu(raw[:, :dim]))
        v_s[g] = silu(raw[:, dim:])

    def rows_of(c):
        return slice(c * CHUNK, (c + 1) * CHUNK)

    for n, (g, c) in enumerate(pieces):
        short = k_s[g, rows_of(c)].astype(BF16)
        gram = dot_nt(short, short)
        place = at(c, g, 1)
        spread = jnp.exp(jnp.minimum(column(c, g, 1) - table_ref[place : place + 1, :], 0.0))
        lower = jnp.where(strict, gram * column(c, g, 0) * spread, 0.0)
        lower_s[n] = lower.astype(BF16)
        inverse_s[n] = (eye - jnp.where(level(1), lower, 0.0)).astype(BF16)

    for i, m in list(enumerate(steps))[1:]:
        odd = [slice(o, o + m) for o in range(m, CHUNK, 2 * m)]
        if m < 16:
            for n in range(len(pieces)):
                half_s[n] = dot(inverse_s[n], lower_s[n] * mask_s[i]).astype(BF16)
            for n in range(len(pieces)):
                inverse_s[n] = inverse_s[n] - dot(half_s[n], inverse_s[n]).astype(BF16)
        else:
            for n in range(len(pieces)):
                picked = jnp.concatenate([inverse_s[n, o] for o in odd], axis=0)
                half_s[n, : CHUNK // 2] = dot(picked, lower_s[n] * mask_s[i]).astype(BF16)
            for n in range(len(pieces)):
                change = dot(half_s[n, : CHUNK // 2], inverse_s[n]).astype(BF16)
                for j, o in enumerate(odd):
                    inverse_s[n, o] = inverse_s[n, o] - change[j * m : (j + 1) * m]

    terms = []
    for n, (g, c) in enumerate(pieces):
        keys, values = k_s[g, rows_of(c)], v_s[g, rows_of(c)]
        strength, total_log = column(c, g, 0), column(c, g, 1)
        last = total_log[CHUNK - 1 : CHUNK]
        off = inverse_s[n] * mask_s[len(steps)]
        source = jnp.concatenate([keys * (strength * jnp.exp(total_log)), values * strength], axis=1)
        solved = source + dot(off, source.astype(BF16))
        faded = (keys * jnp.exp(last - total_log)).astype(BF16)
        change = dot_tn(faded, solved.astype(BF16))
        terms.append((change[:, :dim], change[:, dim:], jnp.exp(last)))

    bit = lax.axis_index("sp") % 2
    half = seqs // 2
    per = chunks // seqs
    for g in range(group):
        maps = []
        for s in range(seqs):
            mine = terms[g * chunks + s * per : g * chunks + (s + 1) * per]
            eraser, target, decay = mine[0]
            held_a, held_b = decay * eye - eraser, target
            for eraser, target, decay in mine[1:]:
                change = dot(
                    eraser.astype(BF16), jnp.concatenate([held_a, held_b], axis=1).astype(BF16)
                )
                held_a = decay * held_a - change[:, :dim]
                held_b = decay * held_b - change[:, dim:] + target
            maps.append((held_a, held_b))
        for s in range(half):
            for part in range(2):
                one, two = maps[s][part], maps[s + half][part]
                rows = slice(part * dim, (part + 1) * dim)
                keep_ref[s * group + g, rows, :] = jnp.where(bit == 0, one, two)
                send_ref[s * group + g, rows, :] = jnp.where(bit == 0, two, one)


def local_maps(x, wk, wv, small, heads, own_heads, dim, table=None):
    seqs, span, width = x.shape
    count = seqs * span
    group = len(own_heads)
    pieces = group * count // CHUNK
    square = (CHUNK, CHUNK)
    result = pltpu.VMEM((seqs // 2 * group, 2 * dim, dim), F32)
    scratch = [
        pltpu.VMEM((group, count, dim), F32),
        pltpu.VMEM((group, count, dim), F32),
        pltpu.VMEM((pieces,) + square, BF16),
        pltpu.VMEM((pieces,) + square, BF16),
        pltpu.VMEM((pieces,) + square, BF16),
        pltpu.VMEM((CHUNK.bit_length(),) + square, BF16),
    ]
    first = table is None
    if first:
        rows = -(-2 * heads * (count // CHUNK) // PAD) * PAD
        scratch += [pltpu.VMEM(x.shape, BF16), pltpu.VMEM((group, width, 2 * dim), BF16)]
        scratch += [pltpu.VMEM(a.shape, a.dtype) for a in small]
        scratch.append(pltpu.SemaphoreType.DMA((seqs + len(small) + 2 * group,)))
        operands = [pltpu.with_memory_space_constraint(a, pltpu.HBM) for a in (x, wk, wv, *small)]
        in_specs = [pl.BlockSpec(memory_space=pltpu.HBM)] * len(operands)
        results = [result, result, pltpu.VMEM((rows, CHUNK), F32)]
    else:
        operands = [x, wk, wv, table]
        in_specs = [WHOLE] * 4
        results = [result, result]
    return pl.pallas_call(
        lambda *refs: local_maps_kernel(*refs, heads=heads, own_heads=own_heads, first=first),
        in_specs=in_specs,
        out_specs=[WHOLE] * len(results),
        out_shape=results,
        scratch_shapes=scratch,
        compiler_params=pltpu.CompilerParams(vmem_limit_bytes=24 * 2**20),
        name="local_maps",
    )(*operands)


def new_token_kernel(
    x_ref, wk_ref, wv_ref, wq_ref, wd_ref, ws_ref, speed_ref, ceil_ref, out_ref
):
    head = pl.program_id(0)
    dim = wk_ref.shape[1]
    x = x_ref[...]
    lane = lax.axis_index("tp") * speed_ref.shape[1] + head

    def project(w_ref):
        return dot(x, w_ref[...]).astype(BF16).astype(F32)

    query = unit(silu(project(wq_ref))) * dim ** (-0.5)
    keys = unit(silu(project(wk_ref)))
    values = silu(project(wv_ref))
    decay_pre = pick_lane(dot_nt(x, wd_ref[...]), lane)
    strength_pre = pick_lane(dot_nt(x, ws_ref[...]), lane)
    fading = jnp.exp(-pick_lane(speed_ref[...], head) * softplus(decay_pre))
    match = jnp.sum(query * keys, axis=-1, keepdims=True) * (
        pick_lane(ceil_ref[...], head) * jax.nn.sigmoid(strength_pre)
    )
    items = [query, keys, values, jnp.broadcast_to(fading, query.shape), jnp.broadcast_to(match, query.shape)]
    for s in range(x.shape[0]):
        for i, item in enumerate(items):
            out_ref[s, 0, i : i + 1, :] = item[s : s + 1]


def new_token(x, wk, wv, wq, wd, ws, speeds, ceilings, dim):
    seqs, width = x.shape
    heads = speeds.shape[0]
    constant = lambda *shape: pl.BlockSpec(shape, lambda h: (0,) * len(shape))
    column = pl.BlockSpec((width, dim), lambda h: (0, h))
    return pl.pallas_call(
        new_token_kernel,
        grid=(heads,),
        in_specs=[
            constant(*x.shape), column, column, column, constant(wd.shape[1], width),
            constant(ws.shape[1], width), constant(1, heads), constant(1, heads),
        ],
        out_specs=pl.BlockSpec((seqs, 1, PAD, dim), lambda h: (0, h, 0, 0)),
        out_shape=pltpu.VMEM((seqs, heads, PAD, dim), F32),
        compiler_params=LIMIT,
        name="new_token",
    )(x, wk, wv, wq, wd.T, ws.T, speeds.reshape(1, -1), ceilings.reshape(1, -1))


def joined(keep, got, bit, dim):
    early = jnp.where(bit == 0, keep, got)
    late = jnp.where(bit == 0, got, keep)
    early = jnp.concatenate([early[:dim], early[dim:]], axis=1)
    both = dot3(late[:dim], early)
    return both[:, :dim], both[:, dim:] + late[dim:]


def join_kernel(keep_ref, got_ref, *outs, stage, split):
    states, rows, dim = keep_ref.shape
    place = lax.axis_index("sp")
    bit = (place >> stage) % 2
    half = states // 2 if split else states
    following = (place >> (stage + 1)) % 2
    for which, out in enumerate(outs):
        for i in range(half):
            at = i + half * (following ^ which) if split else i
            out_a, out_b = joined(keep_ref[at], got_ref[at], bit, dim)
            out[i, :dim, :] = out_a
            out[i, dim:, :] = out_b


def join(keep, got, stage, split):
    states, rows, dim = keep.shape
    count = states // 2 if split else states
    shape = pltpu.VMEM((count, rows, dim), F32)
    return pl.pallas_call(
        lambda *refs: join_kernel(*refs, stage=stage, split=split),
        in_specs=[WHOLE, WHOLE],
        out_specs=[WHOLE] * (2 if split else 1),
        out_shape=[shape] * (2 if split else 1),
        compiler_params=LIMIT,
        name="join",
    )(keep, got)


def state_of(index, place, seqs, heads, split_bits):
    states = seqs * heads
    base = 0
    for b in range(split_bits):
        states //= 2
        base = base + ((place >> b) % 2) * states
    at = base + index
    return at // heads, at % heads


def pack_kernel(keep_ref, got_ref, token_ref, own_ref, send_ref, *, stage, split_bits, own_heads):
    states, rows, dim = keep_ref.shape
    seqs = token_ref.shape[0]
    place = lax.axis_index("sp")
    bit = (place >> stage) % 2
    right = (place >> (stage + 1)) % 2 == 1
    half = dim // 2
    for i in range(states):
        s, h = state_of(i, place, seqs, len(own_heads), split_bits)
        out_a, out_b = joined(keep_ref[i], got_ref[i], bit, dim)
        token = token_ref[s, h + own_heads[0]][:2]
        reads = dot3(jnp.concatenate([token, token, token, token], axis=0), jnp.concatenate([out_a, out_b], axis=1))
        tail = jnp.concatenate([reads[:2, :dim], reads[:2, dim:], reads[:4, :dim]], axis=0)
        own_ref[i, :half, :] = jnp.where(right, out_a[half:], out_b[:half])
        own_ref[i, half:dim, :] = jnp.where(right, out_b[half:], out_b[half:])
        own_ref[i, dim:, :] = tail
        send_ref[i, :half, :] = jnp.where(right, out_a[:half], out_b[:half])
        send_ref[i, half:dim, :] = jnp.where(right, out_b[:half], out_b[half:])
        send_ref[i, dim:, :] = tail


def pack(keep, got, token, stage, split_bits, own_heads):
    states, rows, dim = keep.shape
    shape = pltpu.VMEM((states, dim + PAD, dim), F32)
    return pl.pallas_call(
        lambda *refs: pack_kernel(
            *refs, stage=stage, split_bits=split_bits, own_heads=own_heads
        ),
        in_specs=[WHOLE] * 3,
        out_specs=[WHOLE] * 2,
        out_shape=[shape] * 2,
        compiler_params=LIMIT,
        name="pack",
    )(keep, got, token)


def finish_kernel(*refs, groups, stage, split_bits, block):
    count = len(groups)
    owns, gots = refs[:count], refs[count : 2 * count]
    token_ref, gain_ref = refs[2 * count : 2 * count + 2]
    outs, rows_s = refs[2 * count + 2 : -1], refs[-1]
    states, _, dim = owns[0].shape
    seqs = token_ref.shape[0]
    place = lax.axis_index("sp")
    right = (place >> stage) % 2 == 1
    half = dim // 2
    reads = []
    for g, own_heads in enumerate(groups):
        for i in range(states):
            s, h = state_of(i, place, seqs, len(own_heads), split_bits)
            own, got = owns[g][i], gots[g][i]
            state = jnp.where(right, got[:dim], own[:dim])
            later = jnp.where(right, own, got)
            full = dot3(jnp.concatenate([later[:half], later[dim:]], axis=0), state)
            rows_s[g * states + i] = full[:half] + later[half:dim]
            seen = full[half : half + 2] + later[dim + 2 : dim + 4]
            token = token_ref[s, h + own_heads[0]]
            fading, match = token[3:4], token[4:5]
            mixed = fading * (seen[:1] - match * seen[1:2]) + match * token[2:3]
            scale = lax.rsqrt(jnp.mean(mixed * mixed, axis=-1, keepdims=True) + EPS)
            reads.append(mixed * scale * gain_ref[...])
    blocks = half // block
    total = count * states
    for mask, out in enumerate(outs):
        start = ((place ^ mask) % blocks) * block
        for i in range(total):
            out[i * block : (i + 1) * block, :] = rows_s[i, pl.ds(start, block), :]
            out[total * block + i : total * block + i + 1, :] = reads[i]


def finish(owns, gots, token, gain, groups, stage, split_bits, block):
    states, _, dim = owns[0].shape
    total = states * len(groups)
    rows = -(-(total * block + total) // PAD) * PAD
    shape = pltpu.VMEM((rows, dim), F32)
    count = 2**split_bits
    return pl.pallas_call(
        lambda *refs: finish_kernel(
            *refs, groups=groups, stage=stage, split_bits=split_bits, block=block
        ),
        in_specs=[WHOLE] * (2 * len(groups) + 2),
        out_specs=[WHOLE] * count,
        out_shape=[shape] * count,
        scratch_shapes=[pltpu.VMEM((total, dim // 2, dim), F32)],
        compiler_params=LIMIT,
        name="finish",
    )(*owns, *gots, token, gain.reshape(1, -1))


def place_kernel(*refs, groups, count, split_bits, block):
    ins, cache_ref, read_ref, reads_s = refs[:count], refs[count], refs[count + 1], refs[count + 2]
    seqs, heads, _, dim = cache_ref.shape
    total = seqs * heads // count
    states = total // len(groups)
    place = lax.axis_index("sp")
    for mask, got in enumerate(ins):
        for g, own_heads in enumerate(groups):
            for i in range(states):
                s, h = state_of(i, place ^ mask, seqs, len(own_heads), split_bits)
                h = h + own_heads[0]
                n = g * states + i
                cache_ref[s, h] = got[n * block : (n + 1) * block, :].astype(BF16)
                reads_s[pl.ds(s * heads + h, 1), :] = got[total * block + n : total * block + n + 1, :]
    for h in range(heads):
        rows = [reads_s[s * heads + h : s * heads + h + 1, :] for s in range(seqs)]
        read_ref[:, h * dim : (h + 1) * dim] = jnp.concatenate(rows, axis=0).astype(BF16)


def place_outputs(parts, groups, seqs, heads, dim, block, split_bits):
    count = len(parts)
    return pl.pallas_call(
        lambda *refs: place_kernel(
            *refs, groups=groups, count=count, split_bits=split_bits, block=block
        ),
        in_specs=[WHOLE] * count,
        out_specs=[WHOLE] * 2,
        out_shape=[
            jax.ShapeDtypeStruct((seqs, heads, block, dim), BF16),
            jax.ShapeDtypeStruct((seqs, heads * dim), BF16),
        ],
        scratch_shapes=[pltpu.VMEM((seqs * heads, dim), F32)],
        compiler_params=LIMIT,
        name="place_outputs",
    )(*parts)


def on_device(
    prompt_elements, address_weights, content_weights, lookup_weights, forgetting_weights,
    update_intensity_weights, forgetting_speeds, update_intensity_ceiling, forgetting_multiplier,
    spike_offsets, upcoming_element_vector, retrieval_rms_multiplier,
):
    seqs = prompt_elements.shape[0]
    dim = retrieval_rms_multiplier.shape[0]
    heads = forgetting_speeds.shape[0]
    places = lax.axis_size("sp")
    stages = places.bit_length() - 1
    block = dim // places

    def exchange(values, mask):
        got = lax.ppermute(values, "sp", [(i, i ^ mask) for i in range(places)])
        return pltpu.with_memory_space_constraint(got, pltpu.VMEM)

    parts = 2 if heads % 2 == 0 else 1
    size = heads // parts
    groups = [list(range(g * size, (g + 1) * size)) for g in range(parts)]

    def flat_row(values):
        return jnp.concatenate([values] * (2 if heads == 1 else 1)).reshape(1, -1)

    small = (
        forgetting_weights.T, update_intensity_weights.T, flat_row(forgetting_speeds),
        flat_row(update_intensity_ceiling), forgetting_multiplier.transpose(0, 2, 1),
        spike_offsets.transpose(0, 2, 1),
    )
    table = None
    flows = []
    for own_heads in groups:
        results = local_maps(
            prompt_elements, address_weights, content_weights, small, heads, own_heads, dim, table
        )
        if table is None:
            table = results[2]
        flows.append([results[0], exchange(results[1], 1)])
    token = new_token(
        upcoming_element_vector, address_weights, content_weights, lookup_weights,
        forgetting_weights, update_intensity_weights, forgetting_speeds,
        update_intensity_ceiling, dim,
    )
    states = seqs * size // 2
    split_bits = 1
    for stage in range(stages - 2):
        split = states % 2 == 0 and split_bits == stage + 1
        for flow in flows:
            joint = join(flow[0], flow[1], stage, split)
            flow[:] = joint[0], exchange(joint[-1], 2 ** (stage + 1))
        if split:
            states //= 2
            split_bits += 1
    for own_heads, flow in zip(groups, flows):
        own, send = pack(flow[0], flow[1], token, stages - 2, split_bits, own_heads)
        flow[:] = own, exchange(send, 2 ** (stages - 1))
    pieces = finish(
        [flow[0] for flow in flows], [flow[1] for flow in flows], token,
        retrieval_rms_multiplier, groups, stages - 1, split_bits, block,
    )
    pieces = [piece if mask == 0 else exchange(piece, mask) for mask, piece in enumerate(pieces)]
    cache, read = place_outputs(pieces, groups, seqs, heads, dim, block, split_bits)
    return cache, read


def solution(mesh):
    in_specs = (
        P("gr", "sp", None),
        P(None, "tp"),
        P(None, "tp"),
        P(None, "tp"),
        P(),
        P(),
        P("tp"),
        P("tp"),
        P("gr", "sp", "tp"),
        P("gr", "sp", "tp"),
        P("gr", None),
        P(),
    )
    out_specs = (P("gr", "tp", "sp", None), P("gr", "tp"))
    return jax.shard_map(
        on_device, mesh=mesh, in_specs=in_specs, out_specs=out_specs, check_vma=False
    )
```

```python
import jax
import jax.numpy as jnp
from jax import lax
from jax.experimental import pallas as pl
from jax.experimental.pallas import tpu as pltpu
from jax.sharding import PartitionSpec as P


EPS = 1e-06
CHUNK = 128
PAD = 8
F32 = jnp.float32
BF16 = jnp.bfloat16
WHOLE = pl.BlockSpec(memory_space=pltpu.VMEM)
LIMIT = pltpu.CompilerParams(vmem_limit_bytes=16 * 2**20)


def dot(a, b):
    return jnp.dot(a, b, preferred_element_type=F32)


def dot_nt(a, b):
    return lax.dot_general(a, b, (((1,), (1,)), ((), ())), preferred_element_type=F32)


def dot_tn(a, b):
    return lax.dot_general(a, b, (((0,), (0,)), ((), ())), preferred_element_type=F32)


def halves(a):
    high = a.astype(BF16)
    return high, (a - high.astype(F32)).astype(BF16)


def dot3(a, b):
    ah, al = halves(a)
    bh, bl = halves(b)
    return dot(ah, bh) + dot(ah, bl) + dot(al, bh)


def silu(values):
    return values * jax.nn.sigmoid(values)


def unit(values):
    return values * lax.rsqrt(jnp.sum(values * values, axis=-1, keepdims=True) + EPS)


def softplus(values):
    return jnp.maximum(values, 0.0) + jnp.log1p(jnp.exp(-jnp.abs(values)))


def pick_lane(values, lane):
    places = lax.broadcasted_iota(jnp.int32, values.shape, 1)
    return jnp.sum(jnp.where(places == lane, values, 0.0), axis=1, keepdims=True)


def gate_tables(x, wd, ws, speeds, ceilings, mult, spike, heads, upper):
    total = wd.shape[0]
    rates = jnp.concatenate([wd.astype(F32), ws.astype(F32)], axis=0)
    both = dot_nt(rates.astype(BF16), x)
    shard = lax.axis_index("tp")
    row = lax.broadcasted_iota(jnp.int32, (heads, heads), 0)
    col = lax.broadcasted_iota(jnp.int32, (heads, heads), 1)

    def mine(full):
        part = full[:heads]
        for t in range(1, total // heads):
            part = jnp.where(shard == t, full[t * heads : (t + 1) * heads], part)
        return part

    def upright(values):
        return jnp.sum(jnp.where(row == col, values[:, :heads], 0.0), axis=1, keepdims=True)

    gates = -upright(speeds) * softplus(mine(both[:total])) * mult + spike
    beta = upright(ceilings) * jax.nn.sigmoid(mine(both[total:]))
    rows = []
    for c in range(x.shape[0] // CHUNK):
        lanes = slice(c * CHUNK, (c + 1) * CHUNK)
        rows.append(beta[:, lanes])
        rows.append(
            jnp.dot(gates[:, lanes], upper, precision=lax.Precision.HIGHEST, preferred_element_type=F32)
        )
    fill = -sum(r.shape[0] for r in rows) % PAD
    if fill:
        rows.append(jnp.zeros((fill, CHUNK), F32))
    return jnp.concatenate(rows, axis=0)


def local_maps_kernel(*refs, heads, own_heads, first, bits):
    targets = 2**bits
    if first:
        x_hbm, wk_hbm, wv_hbm = refs[:3]
        small_hbm = refs[3:9]
        table_ref, x_s, w_s = refs[9:12]
        rest = refs[12:]
    else:
        x_s, w_s, table_ref = refs[:3]
        rest = refs[3:]
    outs, rest = rest[:targets], rest[targets:]
    k_s, v_s, lower_s, inverse_s, half_s, mask_s, map_s = rest[:7]
    small_s, sems = rest[7:-1], rest[-1]
    seqs, span, width = x_s.shape
    dim = k_s.shape[-1]
    count = seqs * span
    chunks = count // CHUNK
    group = len(own_heads)
    steps = [2**i for i in range(CHUNK.bit_length() - 1)]

    if first:
        copies = [pltpu.make_async_copy(x_hbm.at[s], x_s.at[s], sems.at[s]) for s in range(seqs)]
        for i, (source, target) in enumerate(zip(small_hbm, small_s)):
            copies.append(pltpu.make_async_copy(source, target, sems.at[seqs + i]))
        base = len(copies)
        for h in range(heads):
            for i, w_hbm in enumerate((wk_hbm, wv_hbm)):
                copies.append(
                    pltpu.make_async_copy(
                        w_hbm.at[:, pl.ds(h * dim, dim)],
                        w_s.at[h, :, pl.ds(i * dim, dim)],
                        sems.at[base + 2 * h + i],
                    )
                )
        for copy in copies:
            copy.start()

    row = lax.broadcasted_iota(jnp.int32, (CHUNK, CHUNK), 0)
    col = lax.broadcasted_iota(jnp.int32, (CHUNK, CHUNK), 1)
    strict = row > col
    eye = jnp.where(row == col, 1.0, 0.0)

    def level(m):
        return (row // (2 * m) == col // (2 * m)) & (row // m != col // m)

    for i, m in enumerate(steps):
        mask_s[i] = jnp.where(level(m), 1.0, 0.0).astype(BF16)
    mask_s[len(steps)] = jnp.where(strict, 1.0, 0.0).astype(BF16)

    if first:
        for copy in copies[:base]:
            copy.wait()
    flat = x_s[...].reshape(count, width)
    if first:
        wd, ws, speeds, ceilings = (ref[...] for ref in small_s[:4])
        mult, spike = (
            jnp.concatenate([ref[s] for s in range(seqs)], axis=1) for ref in small_s[4:]
        )
        table_ref[...] = gate_tables(
            flat, wd, ws, speeds, ceilings, mult, spike, heads, jnp.where(row <= col, 1.0, 0.0)
        )
    columns = table_ref[...].T

    def at(c, g, which):
        return (2 * c + which) * heads + own_heads[g]

    def column(c, g, which):
        return jnp.broadcast_to(columns[:, at(c, g, which) : at(c, g, which) + 1], (CHUNK, CHUNK))

    pieces = [(g, c) for g in range(group) for c in range(chunks)]

    for g, h in enumerate(own_heads):
        if first:
            copies[base + 2 * h].wait()
            copies[base + 2 * h + 1].wait()
        raw = dot(flat, w_s[h]).astype(BF16).astype(F32)
        k_s[g] = unit(silu(raw[:, :dim]))
        v_s[g] = silu(raw[:, dim:])

    def rows_of(c):
        return slice(c * CHUNK, (c + 1) * CHUNK)

    for n, (g, c) in enumerate(pieces):
        short = k_s[g, rows_of(c)].astype(BF16)
        gram = dot_nt(short, short)
        place = at(c, g, 1)
        spread = jnp.exp(jnp.minimum(column(c, g, 1) - table_ref[place : place + 1, :], 0.0))
        lower = jnp.where(strict, gram * column(c, g, 0) * spread, 0.0)
        lower_s[n] = lower.astype(BF16)
        inverse_s[n] = (eye - jnp.where(level(1), lower, 0.0)).astype(BF16)

    for i, m in list(enumerate(steps))[1:]:
        odd = [slice(o, o + m) for o in range(m, CHUNK, 2 * m)]
        if m < 16:
            for n in range(len(pieces)):
                half_s[n] = dot(inverse_s[n], lower_s[n] * mask_s[i]).astype(BF16)
            for n in range(len(pieces)):
                inverse_s[n] = inverse_s[n] - dot(half_s[n], inverse_s[n]).astype(BF16)
        else:
            for n in range(len(pieces)):
                picked = jnp.concatenate([inverse_s[n, o] for o in odd], axis=0)
                half_s[n, : CHUNK // 2] = dot(picked, lower_s[n] * mask_s[i]).astype(BF16)
            for n in range(len(pieces)):
                change = dot(half_s[n, : CHUNK // 2], inverse_s[n]).astype(BF16)
                for j, o in enumerate(odd):
                    inverse_s[n, o] = inverse_s[n, o] - change[j * m : (j + 1) * m]

    terms = []
    for n, (g, c) in enumerate(pieces):
        keys, values = k_s[g, rows_of(c)], v_s[g, rows_of(c)]
        strength, total_log = column(c, g, 0), column(c, g, 1)
        last = total_log[CHUNK - 1 : CHUNK]
        off = inverse_s[n] * mask_s[len(steps)]
        source = jnp.concatenate([keys * (strength * jnp.exp(total_log)), values * strength], axis=1)
        solved = source + dot(off, source.astype(BF16))
        faded = (keys * jnp.exp(last - total_log)).astype(BF16)
        change = dot_tn(faded, solved.astype(BF16))
        terms.append((change[:, :dim], change[:, dim:], jnp.exp(last)))

    per = chunks // seqs
    for g in range(group):
        for s in range(seqs):
            mine = terms[g * chunks + s * per : g * chunks + (s + 1) * per]
            eraser, target, decay = mine[0]
            held_a, held_b = decay * eye - eraser, target
            for eraser, target, decay in mine[1:]:
                change = dot(
                    eraser.astype(BF16), jnp.concatenate([held_a, held_b], axis=1).astype(BF16)
                )
                held_a = decay * held_a - change[:, :dim]
                held_b = decay * held_b - change[:, dim:] + target
            map_s[s * group + g, :dim, :] = held_a
            map_s[s * group + g, dim:, :] = held_b
    states = seqs * group >> bits
    place = lax.axis_index("sp")
    for mask, out in enumerate(outs):
        for i in range(states):
            out[i] = map_s[state_index(i, place ^ mask, seqs * group, bits)]
    if first:
        for copy in copies[base + 2 * len(own_heads) :]:
            copy.wait()


def local_maps(x, w, small, heads, own_heads, dim, bits, table=None):
    seqs, span, width = x.shape
    count = seqs * span
    group = len(own_heads)
    pieces = group * count // CHUNK
    square = (CHUNK, CHUNK)
    results = [pltpu.VMEM((seqs * group >> bits, 2 * dim, dim), F32)] * 2**bits
    scratch = [
        pltpu.VMEM((group, count, dim), F32),
        pltpu.VMEM((group, count, dim), F32),
        pltpu.VMEM((pieces,) + square, BF16),
        pltpu.VMEM((pieces,) + square, BF16),
        pltpu.VMEM((pieces,) + square, BF16),
        pltpu.VMEM((CHUNK.bit_length(),) + square, BF16),
        pltpu.VMEM((seqs * group, 2 * dim, dim), F32),
    ]
    first = table is None
    if first:
        rows = -(-2 * heads * (count // CHUNK) // PAD) * PAD
        scratch += [pltpu.VMEM(a.shape, a.dtype) for a in small]
        operands = [pltpu.with_memory_space_constraint(a, pltpu.HBM) for a in (x, *w, *small)]
        in_specs = [pl.BlockSpec(memory_space=pltpu.HBM)] * len(operands)
        results = [
            pltpu.VMEM((rows, CHUNK), F32),
            pltpu.VMEM(x.shape, BF16),
            pltpu.VMEM((heads, width, 2 * dim), BF16),
        ] + results
    else:
        operands = [x, w, table]
        in_specs = [WHOLE] * 3
    scratch.append(pltpu.SemaphoreType.DMA((seqs + len(small) + 2 * heads,)))
    return pl.pallas_call(
        lambda *refs: local_maps_kernel(
            *refs, heads=heads, own_heads=own_heads, first=first, bits=bits
        ),
        in_specs=in_specs,
        out_specs=[WHOLE] * len(results),
        out_shape=results,
        scratch_shapes=scratch,
        compiler_params=pltpu.CompilerParams(vmem_limit_bytes=24 * 2**20),
        name="local_maps",
    )(*operands)


def state_index(index, place, states, bits):
    base = index
    for b in range(bits):
        states //= 2
        base = base + ((place >> b) % 2) * states
    return base


def new_token_kernel(
    x_ref, w_ref, wq_ref, wd_ref, ws_ref, speed_ref, ceil_ref, out_ref, *, groups, bits
):
    seqs, _ = x_ref.shape
    dim = w_ref.shape[2] // 2
    heads = w_ref.shape[0]
    states = seqs * len(groups[0]) >> bits
    place = lax.axis_index("sp")
    x = x_ref[...]
    decay_pre = dot_nt(x, wd_ref[...])
    strength_pre = dot_nt(x, ws_ref[...])
    for g, own_heads in enumerate(groups):
        for i in range(states):
            index = state_index(i, place, seqs * len(own_heads), bits)
            s, head = index // len(own_heads), index % len(own_heads) + own_heads[0]
            lane = lax.axis_index("tp") * heads + head
            raw = dot(x, w_ref[head]).astype(BF16).astype(F32)
            lanes = pl.ds(pl.multiple_of(head * dim, dim), dim)
            query_raw = dot(x, wq_ref[:, lanes]).astype(BF16).astype(F32)
            query = unit(silu(query_raw)) * dim ** (-0.5)
            keys = unit(silu(raw[:, :dim]))
            values = silu(raw[:, dim:])
            fading = jnp.exp(
                -pick_lane(speed_ref[:, :heads], head) * softplus(pick_lane(decay_pre, lane))
            )
            match = jnp.sum(query * keys, axis=-1, keepdims=True) * (
                pick_lane(ceil_ref[:, :heads], head) * jax.nn.sigmoid(pick_lane(strength_pre, lane))
            )
            wide = [jnp.broadcast_to(item, query.shape) for item in (fading, match)]
            for n, item in enumerate([query, keys, values, *wide]):
                chosen = item[:1]
                for t in range(1, seqs):
                    chosen = jnp.where(s == t, item[t : t + 1], chosen)
                out_ref[g * states + i, n : n + 1, :] = chosen


def new_token(x, w, wq, small, groups, bits, dim):
    states = x.shape[0] * len(groups[0]) >> bits
    return pl.pallas_call(
        lambda *refs: new_token_kernel(*refs, groups=groups, bits=bits),
        in_specs=[WHOLE] * 7,
        out_specs=WHOLE,
        out_shape=pltpu.VMEM((states * len(groups), PAD, dim), F32),
        compiler_params=LIMIT,
        name="new_token",
    )(x, w, wq, *small[:4])


def compose(early, late, dim):
    early = jnp.concatenate([early[:dim], early[dim:]], axis=1)
    both = dot3(late[:dim], early)
    return jnp.concatenate([both[:, :dim], both[:, dim:] + late[dim:]], axis=0)


def gathered(refs, order_s, i, low, dim):
    place = lax.axis_index("sp") >> low
    count = len(refs)
    for mask, ref in enumerate(refs):
        order_s[(place % count) ^ mask] = ref[i]
    held = [order_s[n] for n in range(count)]
    while len(held) > 1:
        held = [compose(held[n], held[n + 1], dim) for n in range(0, len(held), 2)]
    return held[0]


def merge_kernel(*refs, low):
    ins, out, order_s = refs[:-2], refs[-2], refs[-1]
    for i in range(out.shape[0]):
        out[i] = gathered(ins, order_s, i, low, out.shape[2])


def merge(parts, low):
    shape = parts[0].shape
    return pl.pallas_call(
        lambda *refs: merge_kernel(*refs, low=low),
        in_specs=[WHOLE] * len(parts),
        out_specs=WHOLE,
        out_shape=pltpu.VMEM(shape, F32),
        scratch_shapes=[pltpu.VMEM((len(parts),) + shape[1:], F32)],
        compiler_params=LIMIT,
        name="merge",
    )(*parts)


def pack_kernel(*refs, count, earlier, low, top, last):
    ins, rest = refs[:count], refs[count:]
    befores, rest = rest[:earlier], rest[earlier:]
    if last:
        token_ref, own_ref, send_ref, order_s = rest
    else:
        own_ref, send_ref, full_ref, order_s = rest
    states, _, dim = ins[0].shape
    right = (lax.axis_index("sp") >> top) % 2 == 1
    half = dim // 2
    fulls = []
    for i in range(states):
        full = gathered(ins, order_s, i, low, dim)
        fulls.append(full)
        out_a, out_b = full[:dim], full[dim:]
        at = i * dim
        own_ref[at : at + half, :] = jnp.where(right, out_a[half:], out_b[:half])
        own_ref[at + half : at + dim, :] = out_b[half:]
        send_ref[at : at + half, :] = jnp.where(right, out_a[:half], out_b[:half])
        send_ref[at + half : at + dim, :] = jnp.where(right, out_b[:half], out_b[half:])
        if not last:
            full_ref[i] = full
    if last:
        everything = [ref[i] for ref in befores for i in range(states)] + fulls
        for n, full in enumerate(everything):
            token = token_ref[n]
            reads = dot3(token, jnp.concatenate([full[:dim], full[dim:]], axis=1))
            tail = jnp.concatenate([reads[:2, :dim], reads[:2, dim:]], axis=0)
            at = states * dim + 4 * n
            own_ref[at : at + 4, :] = tail
            send_ref[at : at + 4, :] = tail


def pack(parts, befores, token, low, top):
    states, rows, dim = parts[0].shape
    last = token is not None
    tail = -(-4 * states * (len(befores) + 1) // PAD) * PAD if last else 0
    shape = pltpu.VMEM((states * dim + tail, dim), F32)
    results = [shape, shape] + ([] if last else [pltpu.VMEM(parts[0].shape, F32)])
    operands = [*parts, *befores] + ([token] if last else [])
    return pl.pallas_call(
        lambda *refs: pack_kernel(
            *refs, count=len(parts), earlier=len(befores), low=low, top=top, last=last
        ),
        in_specs=[WHOLE] * len(operands),
        out_specs=[WHOLE] * len(results),
        out_shape=results,
        scratch_shapes=[pltpu.VMEM((len(parts), rows, dim), F32)],
        compiler_params=LIMIT,
        name="pack",
    )(*operands)


def finish_kernel(*refs, count, states, top, block):
    owns, gots = refs[:count], refs[count : 2 * count]
    token_ref, gain_ref = refs[2 * count : 2 * count + 2]
    outs, rows_s = refs[2 * count + 2 : -1], refs[-1]
    dim = gain_ref.shape[1]
    place = lax.axis_index("sp")
    right = (place >> top) % 2 == 1
    half = dim // 2
    reads = []
    total = count * states
    for n in range(total):
        at = n % states * dim
        own, got = owns[n // states][at : at + dim, :], gots[n // states][at : at + dim, :]
        state = jnp.where(right, got, own)
        later = jnp.where(right, own, got)
        at = states * dim + 4 * n
        tail = jnp.where(right, owns[-1][at : at + 4, :], gots[-1][at : at + 4, :])
        full = dot3(jnp.concatenate([later[:half], tail, tail], axis=0), state)
        rows_s[n] = full[:half] + later[half:]
        seen = full[half : half + 2] + tail[2:]
        token = token_ref[n]
        fading, match = token[3:4], token[4:5]
        mixed = fading * (seen[:1] - match * seen[1:2]) + match * token[2:3]
        scale = lax.rsqrt(jnp.mean(mixed * mixed, axis=-1, keepdims=True) + EPS)
        reads.append(mixed * scale * gain_ref[...])
    blocks = half // block
    for mask, out in enumerate(outs):
        start = ((place ^ mask) % blocks) * block
        for n in range(total):
            out[n * block : (n + 1) * block, :] = rows_s[n, pl.ds(start, block), :]
            out[total * block + n : total * block + n + 1, :] = reads[n]


def finish(owns, gots, token, gain, top, bits, block):
    dim = owns[0].shape[1]
    total = token.shape[0]
    states = total // len(owns)
    rows = -(-(total * block + total) // PAD) * PAD
    return pl.pallas_call(
        lambda *refs: finish_kernel(*refs, count=len(owns), states=states, top=top, block=block),
        in_specs=[WHOLE] * (2 * len(owns) + 2),
        out_specs=[WHOLE] * 2**bits,
        out_shape=[pltpu.VMEM((rows, dim), F32)] * 2**bits,
        scratch_shapes=[pltpu.VMEM((total, dim // 2, dim), F32)],
        compiler_params=LIMIT,
        name="finish",
    )(*owns, *gots, token, gain.reshape(1, -1))


def place_kernel(*refs, groups, bits, block):
    count = 2**bits
    ins, cache_ref, read_ref, reads_s = refs[:count], refs[count], refs[count + 1], refs[count + 2]
    seqs, heads, _, dim = cache_ref.shape
    total = seqs * heads // count
    states = total // len(groups)
    place = lax.axis_index("sp")
    for mask, got in enumerate(ins):
        for g, own_heads in enumerate(groups):
            for i in range(states):
                index = state_index(i, place ^ mask, seqs * len(own_heads), bits)
                s, h = index // len(own_heads), index % len(own_heads) + own_heads[0]
                n = g * states + i
                cache_ref[s, h] = got[n * block : (n + 1) * block, :].astype(BF16)
                reads_s[pl.ds(s * heads + h, 1), :] = got[total * block + n : total * block + n + 1, :]
    for h in range(heads):
        rows = [reads_s[s * heads + h : s * heads + h + 1, :] for s in range(seqs)]
        read_ref[:, h * dim : (h + 1) * dim] = jnp.concatenate(rows, axis=0).astype(BF16)


def place_outputs(parts, groups, seqs, heads, dim, block, bits):
    return pl.pallas_call(
        lambda *refs: place_kernel(*refs, groups=groups, bits=bits, block=block),
        in_specs=[WHOLE] * len(parts),
        out_specs=[WHOLE] * 2,
        out_shape=[
            jax.ShapeDtypeStruct((seqs, heads, block, dim), BF16),
            jax.ShapeDtypeStruct((seqs, heads * dim), BF16),
        ],
        scratch_shapes=[pltpu.VMEM((seqs * heads, dim), F32)],
        compiler_params=LIMIT,
        name="place_outputs",
    )(*parts)


def on_device(
    prompt_elements, address_weights, content_weights, lookup_weights, forgetting_weights,
    update_intensity_weights, forgetting_speeds, update_intensity_ceiling, forgetting_multiplier,
    spike_offsets, upcoming_element_vector, retrieval_rms_multiplier,
):
    seqs = prompt_elements.shape[0]
    dim = retrieval_rms_multiplier.shape[0]
    heads = forgetting_speeds.shape[0]
    places = lax.axis_size("sp")
    stages = places.bit_length() - 1
    block = dim // places

    def exchange(values, mask):
        got = lax.ppermute(values, "sp", [(i, i ^ mask) for i in range(places)])
        return pltpu.with_memory_space_constraint(got, pltpu.VMEM)

    parts = 2 if heads % 2 == 0 else 1
    size = heads // parts
    groups = [list(range(g * size, (g + 1) * size)) for g in range(parts)]

    def flat_row(values):
        return jnp.concatenate([values] * (2 if heads == 1 else 1)).reshape(1, -1)

    small = (
        forgetting_weights.T, update_intensity_weights.T, flat_row(forgetting_speeds),
        flat_row(update_intensity_ceiling), forgetting_multiplier.transpose(0, 2, 1),
        spike_offsets.transpose(0, 2, 1),
    )
    bits = min((seqs * size).bit_length() - 1, stages - 1)
    top = stages - 1
    table = None
    flows = []
    x, w = prompt_elements, (address_weights, content_weights)
    for own_heads in groups:
        results = local_maps(x, w, small, heads, own_heads, dim, bits, table)
        if table is None:
            table, x, w, *results = results
        flows.append([part if m == 0 else exchange(part, m) for m, part in enumerate(results)])
    token = new_token(upcoming_element_vector, w, lookup_weights, small, groups, bits, dim)
    low, span = 0, bits
    while low + span < top:
        for flow in flows:
            joint = merge(flow, low)
            flow[:] = joint, exchange(joint, 2 ** (low + span))
        low, span = low + span, 1
    owns, gots, fulls = [], [], []
    for g, flow in enumerate(flows):
        last = g == len(flows) - 1
        own, send, *full = pack(flow, fulls if last else [], token if last else None, low, top)
        fulls += full
        owns.append(own)
        gots.append(exchange(send, 2**top))
    pieces = finish(owns, gots, token, retrieval_rms_multiplier, top, bits, block)
    pieces = [piece if mask == 0 else exchange(piece, mask) for mask, piece in enumerate(pieces)]
    return tuple(place_outputs(pieces, groups, seqs, heads, dim, block, bits))


def solution(mesh):
    in_specs = (
        P("gr", "sp", None),
        P(None, "tp"),
        P(None, "tp"),
        P(None, "tp"),
        P(),
        P(),
        P("tp"),
        P("tp"),
        P("gr", "sp", "tp"),
        P("gr", "sp", "tp"),
        P("gr", None),
        P(),
    )
    out_specs = (P("gr", "tp", "sp", None), P("gr", "tp"))

    return jax.shard_map(
        on_device, mesh=mesh, in_specs=in_specs, out_specs=out_specs, check_vma=False
    )
```

```python
import jax
import jax.numpy as jnp
from jax import lax
from jax.experimental import pallas as pl
from jax.experimental.pallas import tpu as pltpu
from jax.sharding import PartitionSpec as P


EPS = 1e-06
CHUNK = 128
PAD = 8
F32 = jnp.float32
BF16 = jnp.bfloat16
WHOLE = pl.BlockSpec(memory_space=pltpu.VMEM)
LIMIT = pltpu.CompilerParams(vmem_limit_bytes=16 * 2**20)


def dot(a, b):
    return jnp.dot(a, b, preferred_element_type=F32)


def dot_nt(a, b):
    return lax.dot_general(a, b, (((1,), (1,)), ((), ())), preferred_element_type=F32)


def dot_tn(a, b):
    return lax.dot_general(a, b, (((0,), (0,)), ((), ())), preferred_element_type=F32)


def halves(a):
    high = a.astype(BF16)
    return high, (a - high.astype(F32)).astype(BF16)


def dot3(a, b):
    ah, al = halves(a)
    bh, bl = halves(b)
    return dot(ah, bh) + dot(ah, bl) + dot(al, bh)


def silu(values):
    return values * jax.nn.sigmoid(values)


def unit(values):
    return values * lax.rsqrt(jnp.sum(values * values, axis=-1, keepdims=True) + EPS)


def softplus(values):
    return jnp.maximum(values, 0.0) + jnp.log1p(jnp.exp(-jnp.abs(values)))


def pick_lane(values, lane):
    places = lax.broadcasted_iota(jnp.int32, values.shape, 1)
    return jnp.sum(jnp.where(places == lane, values, 0.0), axis=1, keepdims=True)


def gate_tables(x, wd, ws, speeds, ceilings, mult, spike, heads, upper):
    total = wd.shape[0]
    rates = jnp.concatenate([wd.astype(F32), ws.astype(F32)], axis=0)
    both = dot_nt(rates.astype(BF16), x)
    shard = lax.axis_index("tp")
    row = lax.broadcasted_iota(jnp.int32, (heads, heads), 0)
    col = lax.broadcasted_iota(jnp.int32, (heads, heads), 1)

    def mine(full):
        part = full[:heads]
        for t in range(1, total // heads):
            part = jnp.where(shard == t, full[t * heads : (t + 1) * heads], part)
        return part

    def upright(values):
        return jnp.sum(jnp.where(row == col, values[:, :heads], 0.0), axis=1, keepdims=True)

    gates = -upright(speeds) * softplus(mine(both[:total])) * mult + spike
    beta = upright(ceilings) * jax.nn.sigmoid(mine(both[total:]))
    rows = []
    for c in range(x.shape[0] // CHUNK):
        lanes = slice(c * CHUNK, (c + 1) * CHUNK)
        rows.append(beta[:, lanes])
        rows.append(
            jnp.dot(gates[:, lanes], upper, precision=lax.Precision.HIGHEST, preferred_element_type=F32)
        )
    fill = -sum(r.shape[0] for r in rows) % PAD
    if fill:
        rows.append(jnp.zeros((fill, CHUNK), F32))
    return jnp.concatenate(rows, axis=0)


def local_maps_kernel(*refs, heads, own_heads, first, bits):
    if first:
        x_hbm, wk_hbm, wv_hbm = refs[:3]
        small_hbm, (table_ref, x_s, w_s), rest = refs[3:9], refs[9:12], refs[12:]
    else:
        (x_s, w_s, table_ref), rest = refs[:3], refs[3:]
    outs, rest = rest[: 2**bits], rest[2**bits :]
    source_s, map_s = rest[:2]
    small_s, sems = rest[2:-1], rest[-1]
    seqs, span, width = x_s.shape
    dim = source_s.shape[-1] // 2
    count = seqs * span
    chunks = count // CHUNK
    group = len(own_heads)
    steps = [2**i for i in range(CHUNK.bit_length() - 1)]

    if first:
        copies = [pltpu.make_async_copy(x_hbm.at[s], x_s.at[s], sems.at[s]) for s in range(seqs)]
        for i, (origin, target) in enumerate(zip(small_hbm, small_s)):
            copies.append(pltpu.make_async_copy(origin, target, sems.at[seqs + i]))
        base = len(copies)
        for h in range(heads):
            for i, w_hbm in enumerate((wk_hbm, wv_hbm)):
                copies.append(
                    pltpu.make_async_copy(
                        w_hbm.at[:, pl.ds(h * dim, dim)],
                        w_s.at[h, :, pl.ds(i * dim, dim)],
                        sems.at[base + 2 * h + i],
                    )
                )
        own_copies = copies[base : base + 2 * group]
        other_copies = copies[base + 2 * group :]
        for copy in copies[:base] + own_copies:
            copy.start()

    row = lax.broadcasted_iota(jnp.int32, (CHUNK, CHUNK), 0)
    col = lax.broadcasted_iota(jnp.int32, (CHUNK, CHUNK), 1)
    eye = jnp.where(row == col, 1.0, 0.0)
    upper = jnp.where(row <= col, 1.0, 0.0)

    def level(m):
        return (row // (2 * m) == col // (2 * m)) & (row // m != col // m)

    masks = [jnp.where(level(m), 1.0, 0.0).astype(BF16) for m in steps]
    strict = jnp.where(row > col, 1.0, 0.0).astype(BF16)
    eye_short = eye.astype(BF16)

    if first:
        for copy in copies[:base]:
            copy.wait()
        for copy in other_copies:
            copy.start()
        wd, ws, speeds, ceilings = (ref[...] for ref in small_s[:4])
        mult, spike = (
            jnp.concatenate([ref[s] for s in range(seqs)], axis=1) for ref in small_s[4:]
        )
        table_ref[...] = gate_tables(
            x_s[...].reshape(count, width), wd, ws, speeds, ceilings, mult, spike, heads, upper
        )
        for copy in own_copies:
            copy.wait()
    table = table_ref[...]
    columns = table.T

    def at(c, h, which):
        return (2 * c + which) * heads + h

    def column(c, h, which):
        return jnp.broadcast_to(columns[:, at(c, h, which) : at(c, h, which) + 1], (CHUNK, CHUNK))

    def project(h):
        return dot(x_s[...].reshape(count, width), w_s[h])

    pieces = range(group * chunks)
    lasts, lowers, inverses, fadeds = [], [], [], []

    def prepare(g, raw):
        h = own_heads[g]
        raw = raw.astype(BF16).astype(F32)
        keys_all = unit(silu(raw[:, :dim]))
        values_all = silu(raw[:, dim:])
        for c in range(chunks):
            n = g * chunks + c
            keys = keys_all[c * CHUNK : (c + 1) * CHUNK]
            values = values_all[c * CHUNK : (c + 1) * CHUNK]
            strength, total_log = column(c, h, 0), column(c, h, 1)
            last = total_log[CHUNK - 1 : CHUNK]
            short = keys.astype(BF16)
            gram = dot_nt(short, short)
            place = at(c, h, 1)
            spread = jnp.exp(jnp.minimum(total_log - table[place : place + 1], 0.0))
            lower = (gram * strength * spread).astype(BF16) * strict
            lowers.append(lower)
            inverses.append(eye_short - lower * masks[0])
            source_s[n, :, :dim] = keys * (strength * jnp.exp(total_log))
            source_s[n, :, dim:] = values * strength
            fadeds.append((keys * jnp.exp(last - total_log)).astype(BF16))
            lasts.append(jnp.exp(last))

    raws = [project(h) for h in own_heads]
    for g in range(group):
        prepare(g, raws[g])

    for i, m in list(enumerate(steps))[1:]:
        if m < 16:
            products = [dot(inverses[n], lowers[n] * masks[i]).astype(BF16) for n in pieces]
            inverses = [
                inverses[n] - dot(products[n], inverses[n]).astype(BF16) for n in pieces
            ]
            continue
        odd = [slice(o, o + m) for o in range(m, CHUNK, 2 * m)]
        products = []
        for n in pieces:
            picked = jnp.concatenate([inverses[n][o] for o in odd], axis=0)
            products.append(dot(picked, lowers[n] * masks[i]).astype(BF16))
        for n in pieces:
            change = dot(products[n], inverses[n]).astype(BF16)
            parts = []
            for j, o in enumerate(odd):
                parts.append(inverses[n][o.start - m : o.start])
                parts.append(inverses[n][o] - change[j * m : (j + 1) * m])
            inverses[n] = jnp.concatenate(parts, axis=0)

    terms = []
    for n in pieces:
        off = inverses[n] - eye_short
        source = source_s[n]
        solved = source + dot(off, source.astype(BF16))
        terms.append(dot_tn(fadeds[n], solved.astype(BF16)))

    per = chunks // seqs
    place = lax.axis_index("sp")
    states = seqs * group
    for g in range(group):
        for s in range(seqs):
            n = g * chunks + s * per
            held_a, held_b = lasts[n] * eye - terms[n][:, :dim], terms[n][:, dim:]
            for n in range(n + 1, n + per):
                change = dot(
                    terms[n][:, :dim].astype(BF16),
                    jnp.concatenate([held_a, held_b], axis=1).astype(BF16),
                )
                held_a = lasts[n] * held_a - change[:, :dim]
                held_b = lasts[n] * held_b - change[:, dim:] + terms[n][:, dim:]
            map_s[s * group + g, :dim, :] = held_a
            map_s[s * group + g, dim:, :] = held_b
    for mask, out in enumerate(outs):
        for i in range(states >> bits):
            out[i] = map_s[state_index(i, place ^ mask, states, bits)]
    if first:
        for copy in other_copies:
            copy.wait()


def local_maps(x, w, small, heads, own_heads, dim, bits, table=None):
    seqs, span, width = x.shape
    count = seqs * span
    group = len(own_heads)
    states = seqs * group
    pieces = group * count // CHUNK
    results = [pltpu.VMEM((states >> bits, 2 * dim, dim), F32)] * 2**bits
    scratch = [
        pltpu.VMEM((pieces, CHUNK, 2 * dim), F32),
        pltpu.VMEM((states, 2 * dim, dim), F32),
    ]
    first = table is None
    if first:
        rows = -(-2 * heads * (count // CHUNK) // PAD) * PAD
        scratch += [pltpu.VMEM(a.shape, a.dtype) for a in small]
        operands = [pltpu.with_memory_space_constraint(a, pltpu.HBM) for a in (x, *w, *small)]
        in_specs = [pl.BlockSpec(memory_space=pltpu.HBM)] * len(operands)
        results = [
            pltpu.VMEM((rows, CHUNK), F32),
            pltpu.VMEM(x.shape, BF16),
            pltpu.VMEM((heads, width, 2 * dim), BF16),
        ] + results
    else:
        operands = [x, w, table]
        in_specs = [WHOLE] * 3
    scratch.append(pltpu.SemaphoreType.DMA((seqs + len(small) + 2 * heads,)))
    return pl.pallas_call(
        lambda *refs: local_maps_kernel(
            *refs, heads=heads, own_heads=own_heads, first=first, bits=bits
        ),
        in_specs=in_specs,
        out_specs=[WHOLE] * len(results),
        out_shape=results,
        scratch_shapes=scratch,
        compiler_params=pltpu.CompilerParams(vmem_limit_bytes=24 * 2**20),
        name="local_maps",
    )(*operands)


def state_index(index, place, states, bits):
    base = index
    for b in range(bits):
        states //= 2
        base = base + ((place >> b) % 2) * states
    return base


def new_token_kernel(
    x_ref, w_ref, wq_ref, wd_ref, ws_ref, speed_ref, ceil_ref, out_ref, *, groups, bits
):
    seqs, _ = x_ref.shape
    dim = w_ref.shape[2] // 2
    heads = w_ref.shape[0]
    states = seqs * len(groups[0]) >> bits
    place = lax.axis_index("sp")
    x = x_ref[...]
    decay_pre = dot_nt(x, wd_ref[...])
    strength_pre = dot_nt(x, ws_ref[...])
    for g, own_heads in enumerate(groups):
        for i in range(states):
            index = state_index(i, place, seqs * len(own_heads), bits)
            s, head = index // len(own_heads), index % len(own_heads) + own_heads[0]
            lane = lax.axis_index("tp") * heads + head
            raw = dot(x, w_ref[head]).astype(BF16).astype(F32)
            lanes = pl.ds(pl.multiple_of(head * dim, dim), dim)
            query_raw = dot(x, wq_ref[:, lanes]).astype(BF16).astype(F32)
            query = unit(silu(query_raw)) * dim ** (-0.5)
            keys = unit(silu(raw[:, :dim]))
            values = silu(raw[:, dim:])
            fading = jnp.exp(
                -pick_lane(speed_ref[:, :heads], head) * softplus(pick_lane(decay_pre, lane))
            )
            match = jnp.sum(query * keys, axis=-1, keepdims=True) * (
                pick_lane(ceil_ref[:, :heads], head) * jax.nn.sigmoid(pick_lane(strength_pre, lane))
            )
            wide = [jnp.broadcast_to(item, query.shape) for item in (fading, match)]
            for n, item in enumerate([query, keys, values, *wide]):
                chosen = item[:1]
                for t in range(1, seqs):
                    chosen = jnp.where(s == t, item[t : t + 1], chosen)
                out_ref[g * states + i, n : n + 1, :] = chosen


def new_token(x, w, wq, small, groups, bits, dim):
    states = x.shape[0] * len(groups[0]) >> bits
    return pl.pallas_call(
        lambda *refs: new_token_kernel(*refs, groups=groups, bits=bits),
        in_specs=[WHOLE] * 7,
        out_specs=WHOLE,
        out_shape=pltpu.VMEM((states * len(groups), PAD, dim), F32),
        compiler_params=LIMIT,
        name="new_token",
    )(x, w, wq, *small[:4])


def compose(early, late, dim):
    early = jnp.concatenate([early[:dim], early[dim:]], axis=1)
    both = dot3(late[:dim], early)
    return jnp.concatenate([both[:, :dim], both[:, dim:] + late[dim:]], axis=0)


def gathered(refs, order_s, i, low, dim):
    place = lax.axis_index("sp") >> low
    count = len(refs)
    for mask, ref in enumerate(refs):
        order_s[(place % count) ^ mask] = ref[i]
    held = [order_s[n] for n in range(count)]
    while len(held) > 1:
        held = [compose(held[n], held[n + 1], dim) for n in range(0, len(held), 2)]
    return held[0]


def merge_kernel(*refs, low):
    ins, out, order_s = refs[:-2], refs[-2], refs[-1]
    for i in range(out.shape[0]):
        out[i] = gathered(ins, order_s, i, low, out.shape[2])


def merge(parts, low):
    shape = parts[0].shape
    return pl.pallas_call(
        lambda *refs: merge_kernel(*refs, low=low),
        in_specs=[WHOLE] * len(parts),
        out_specs=WHOLE,
        out_shape=pltpu.VMEM(shape, F32),
        scratch_shapes=[pltpu.VMEM((len(parts),) + shape[1:], F32)],
        compiler_params=LIMIT,
        name="merge",
    )(*parts)


def pack_kernel(*refs, count, earlier, low, top, last):
    ins, rest = refs[:count], refs[count:]
    befores, rest = rest[:earlier], rest[earlier:]
    if last:
        token_ref, own_ref, send_ref, order_s = rest
    else:
        own_ref, send_ref, full_ref, order_s = rest
    states, _, dim = ins[0].shape
    right = (lax.axis_index("sp") >> top) % 2 == 1
    half = dim // 2
    fulls = []
    for i in range(states):
        full = gathered(ins, order_s, i, low, dim)
        fulls.append(full)
        out_a, out_b = full[:dim], full[dim:]
        at = i * dim
        own_ref[at : at + half, :] = jnp.where(right, out_a[half:], out_b[:half])
        own_ref[at + half : at + dim, :] = out_b[half:]
        send_ref[at : at + half, :] = jnp.where(right, out_a[:half], out_b[:half])
        send_ref[at + half : at + dim, :] = jnp.where(right, out_b[:half], out_b[half:])
        if not last:
            full_ref[i] = full
    if last:
        everything = [ref[i] for ref in befores for i in range(states)] + fulls
        for n, full in enumerate(everything):
            token = token_ref[n]
            reads = dot3(token, jnp.concatenate([full[:dim], full[dim:]], axis=1))
            tail = jnp.concatenate([reads[:2, :dim], reads[:2, dim:]], axis=0)
            at = states * dim + 4 * n
            own_ref[at : at + 4, :] = tail
            send_ref[at : at + 4, :] = tail


def pack(parts, befores, token, low, top):
    states, rows, dim = parts[0].shape
    last = token is not None
    tail = -(-4 * states * (len(befores) + 1) // PAD) * PAD if last else 0
    shape = pltpu.VMEM((states * dim + tail, dim), F32)
    results = [shape, shape] + ([] if last else [pltpu.VMEM(parts[0].shape, F32)])
    operands = [*parts, *befores] + ([token] if last else [])
    return pl.pallas_call(
        lambda *refs: pack_kernel(
            *refs, count=len(parts), earlier=len(befores), low=low, top=top, last=last
        ),
        in_specs=[WHOLE] * len(operands),
        out_specs=[WHOLE] * len(results),
        out_shape=results,
        scratch_shapes=[pltpu.VMEM((len(parts), rows, dim), F32)],
        compiler_params=LIMIT,
        name="pack",
    )(*operands)


def finish_kernel(*refs, count, states, top, block):
    owns, gots = refs[:count], refs[count : 2 * count]
    token_ref, gain_ref = refs[2 * count : 2 * count + 2]
    outs, rows_s = refs[2 * count + 2 : -1], refs[-1]
    dim = gain_ref.shape[1]
    place = lax.axis_index("sp")
    right = (place >> top) % 2 == 1
    half = dim // 2
    reads = []
    total = count * states
    for n in range(total):
        at = n % states * dim
        own, got = owns[n // states][at : at + dim, :], gots[n // states][at : at + dim, :]
        state = jnp.where(right, got, own)
        later = jnp.where(right, own, got)
        at = states * dim + 4 * n
        tail = jnp.where(right, owns[-1][at : at + 4, :], gots[-1][at : at + 4, :])
        full = dot3(jnp.concatenate([later[:half], tail, tail], axis=0), state)
        rows_s[n] = full[:half] + later[half:]
        seen = full[half : half + 2] + tail[2:]
        token = token_ref[n]
        fading, match = token[3:4], token[4:5]
        mixed = fading * (seen[:1] - match * seen[1:2]) + match * token[2:3]
        scale = lax.rsqrt(jnp.mean(mixed * mixed, axis=-1, keepdims=True) + EPS)
        reads.append(mixed * scale * gain_ref[...])
    blocks = half // block
    for mask, out in enumerate(outs):
        start = ((place ^ mask) % blocks) * block
        for n in range(total):
            out[n * block : (n + 1) * block, :] = rows_s[n, pl.ds(start, block), :]
            out[total * block + n : total * block + n + 1, :] = reads[n]


def finish(owns, gots, token, gain, top, bits, block):
    dim = owns[0].shape[1]
    total = token.shape[0]
    states = total // len(owns)
    rows = -(-(total * block + total) // PAD) * PAD
    return pl.pallas_call(
        lambda *refs: finish_kernel(*refs, count=len(owns), states=states, top=top, block=block),
        in_specs=[WHOLE] * (2 * len(owns) + 2),
        out_specs=[WHOLE] * 2**bits,
        out_shape=[pltpu.VMEM((rows, dim), F32)] * 2**bits,
        scratch_shapes=[pltpu.VMEM((total, dim // 2, dim), F32)],
        compiler_params=LIMIT,
        name="finish",
    )(*owns, *gots, token, gain.reshape(1, -1))


def place_kernel(*refs, groups, bits, block):
    count = 2**bits
    ins, cache_ref, read_ref, reads_s = refs[:count], refs[count], refs[count + 1], refs[count + 2]
    seqs, heads, _, dim = cache_ref.shape
    total = seqs * heads // count
    states = total // len(groups)
    place = lax.axis_index("sp")
    for mask, got in enumerate(ins):
        for g, own_heads in enumerate(groups):
            for i in range(states):
                index = state_index(i, place ^ mask, seqs * len(own_heads), bits)
                s, h = index // len(own_heads), index % len(own_heads) + own_heads[0]
                n = g * states + i
                cache_ref[s, h] = got[n * block : (n + 1) * block, :].astype(BF16)
                reads_s[pl.ds(s * heads + h, 1), :] = got[total * block + n : total * block + n + 1, :]
    for h in range(heads):
        rows = [reads_s[s * heads + h : s * heads + h + 1, :] for s in range(seqs)]
        read_ref[:, h * dim : (h + 1) * dim] = jnp.concatenate(rows, axis=0).astype(BF16)


def place_outputs(parts, groups, seqs, heads, dim, block, bits):
    return pl.pallas_call(
        lambda *refs: place_kernel(*refs, groups=groups, bits=bits, block=block),
        in_specs=[WHOLE] * len(parts),
        out_specs=[WHOLE] * 2,
        out_shape=[
            jax.ShapeDtypeStruct((seqs, heads, block, dim), BF16),
            jax.ShapeDtypeStruct((seqs, heads * dim), BF16),
        ],
        scratch_shapes=[pltpu.VMEM((seqs * heads, dim), F32)],
        compiler_params=LIMIT,
        name="place_outputs",
    )(*parts)


def on_device(
    prompt_elements, address_weights, content_weights, lookup_weights, forgetting_weights,
    update_intensity_weights, forgetting_speeds, update_intensity_ceiling, forgetting_multiplier,
    spike_offsets, upcoming_element_vector, retrieval_rms_multiplier,
):
    seqs = prompt_elements.shape[0]
    dim = retrieval_rms_multiplier.shape[0]
    heads = forgetting_speeds.shape[0]
    places = lax.axis_size("sp")
    stages = places.bit_length() - 1
    block = dim // places

    def exchange(values, mask):
        got = lax.ppermute(values, "sp", [(i, i ^ mask) for i in range(places)])
        return pltpu.with_memory_space_constraint(got, pltpu.VMEM)

    parts = 2 if heads % 2 == 0 else 1
    size = heads // parts
    groups = [list(range(g * size, (g + 1) * size)) for g in range(parts)]

    def flat_row(values):
        return jnp.concatenate([values] * (2 if heads == 1 else 1)).reshape(1, -1)

    small = (
        forgetting_weights.T, update_intensity_weights.T, flat_row(forgetting_speeds),
        flat_row(update_intensity_ceiling), forgetting_multiplier.transpose(0, 2, 1),
        spike_offsets.transpose(0, 2, 1),
    )
    bits = min((seqs * size).bit_length() - 1, stages - 1)
    top = stages - 1
    table = None
    flows = []
    x, w = prompt_elements, (address_weights, content_weights)
    for own_heads in groups:
        results = local_maps(x, w, small, heads, own_heads, dim, bits, table)
        if table is None:
            table, x, w, *results = results
        flow = [results[0]] + [None] * (len(results) - 1)
        for m in range(1, len(results)):
            flow[m] = exchange(results[m], m)
        flows.append(flow)
    token = new_token(upcoming_element_vector, w, lookup_weights, small, groups, bits, dim)
    low, span = 0, bits
    while low + span < top:
        for flow in flows:
            joint = merge(flow, low)
            flow[:] = joint, exchange(joint, 2 ** (low + span))
        low, span = low + span, 1
    owns, gots, fulls = [], [], []
    for g, flow in enumerate(flows):
        last = g == len(flows) - 1
        own, send, *full = pack(flow, fulls if last else [], token if last else None, low, top)
        fulls += full
        owns.append(own)
        gots.append(exchange(send, 2**top))
    pieces = finish(owns, gots, token, retrieval_rms_multiplier, top, bits, block)
    pieces = [piece if mask == 0 else exchange(piece, mask) for mask, piece in enumerate(pieces)]
    return tuple(place_outputs(pieces, groups, seqs, heads, dim, block, bits))


def solution(mesh):
    in_specs = (
        P("gr", "sp", None),
        P(None, "tp"),
        P(None, "tp"),
        P(None, "tp"),
        P(),
        P(),
        P("tp"),
        P("tp"),
        P("gr", "sp", "tp"),
        P("gr", "sp", "tp"),
        P("gr", None),
        P(),
    )
    out_specs = (P("gr", "tp", "sp", None), P("gr", "tp"))

    return jax.shard_map(
        on_device, mesh=mesh, in_specs=in_specs, out_specs=out_specs, check_vma=False
    )
```

```python
import jax
import jax.numpy as jnp
from jax import lax
from jax.experimental import pallas as pl
from jax.experimental.pallas import tpu as pltpu
from jax.sharding import PartitionSpec as P


EPS = 1e-06
CHUNK = 128
PAD = 8
F32 = jnp.float32
BF16 = jnp.bfloat16
WHOLE = pl.BlockSpec(memory_space=pltpu.VMEM)
LIMIT = pltpu.CompilerParams(vmem_limit_bytes=16 * 2**20)


def dot(a, b):
    return jnp.dot(a, b, preferred_element_type=F32)


def dot_nt(a, b):
    return lax.dot_general(a, b, (((1,), (1,)), ((), ())), preferred_element_type=F32)


def dot_tn(a, b):
    return lax.dot_general(a, b, (((0,), (0,)), ((), ())), preferred_element_type=F32)


def halves(a):
    high = a.astype(BF16)
    return high, (a - high.astype(F32)).astype(BF16)


def dot3(a, b):
    ah, al = halves(a)
    bh, bl = halves(b)
    return dot(ah, bh) + dot(ah, bl) + dot(al, bh)


def silu(values):
    return values * jax.nn.sigmoid(values)


def unit(values):
    return values * lax.rsqrt(jnp.sum(values * values, axis=-1, keepdims=True) + EPS)


def softplus(values):
    return jnp.maximum(values, 0.0) + jnp.log1p(jnp.exp(-jnp.abs(values)))


def pick_lane(values, lane):
    places = lax.broadcasted_iota(jnp.int32, values.shape, 1)
    return jnp.sum(jnp.where(places == lane, values, 0.0), axis=1, keepdims=True)


def gate_tables(x, wd, ws, speeds, ceilings, mult, spike, heads, upper):
    total = wd.shape[0]
    rates = jnp.concatenate([wd.astype(F32), ws.astype(F32)], axis=0)
    both = dot_nt(rates.astype(BF16), x)
    shard = lax.axis_index("tp")
    row = lax.broadcasted_iota(jnp.int32, (heads, heads), 0)
    col = lax.broadcasted_iota(jnp.int32, (heads, heads), 1)

    def mine(full):
        part = full[:heads]
        for t in range(1, total // heads):
            part = jnp.where(shard == t, full[t * heads : (t + 1) * heads], part)
        return part

    def upright(values):
        return jnp.sum(jnp.where(row == col, values[:, :heads], 0.0), axis=1, keepdims=True)

    gates = -upright(speeds) * softplus(mine(both[:total])) * mult + spike
    beta = upright(ceilings) * jax.nn.sigmoid(mine(both[total:]))
    rows = []
    for c in range(x.shape[0] // CHUNK):
        lanes = slice(c * CHUNK, (c + 1) * CHUNK)
        rows.append(beta[:, lanes])
        rows.append(
            jnp.dot(gates[:, lanes], upper, precision=lax.Precision.HIGHEST, preferred_element_type=F32)
        )
    fill = -sum(r.shape[0] for r in rows) % PAD
    if fill:
        rows.append(jnp.zeros((fill, CHUNK), F32))
    return jnp.concatenate(rows, axis=0)


def local_maps_kernel(*refs, heads, own_heads, first, bits):
    if first:
        x_hbm, wk_hbm, wv_hbm = refs[:3]
        small_hbm, (table_ref, x_s, w_s), rest = refs[3:9], refs[9:12], refs[12:]
    else:
        (x_s, w_s, table_ref), rest = refs[:3], refs[3:]
    outs, rest = rest[: 2**bits], rest[2**bits :]
    source_s, map_s = rest[:2]
    small_s, sems = rest[2:-1], rest[-1]
    seqs, span, width = x_s.shape
    dim = source_s.shape[-1] // 2
    count = seqs * span
    chunks = count // CHUNK
    group = len(own_heads)
    steps = [2**i for i in range(CHUNK.bit_length() - 1)]

    if first:
        copies = [pltpu.make_async_copy(x_hbm.at[s], x_s.at[s], sems.at[s]) for s in range(seqs)]
        for i, (origin, target) in enumerate(zip(small_hbm, small_s)):
            copies.append(pltpu.make_async_copy(origin, target, sems.at[seqs + i]))
        base = len(copies)
        for h in range(heads):
            for i, w_hbm in enumerate((wk_hbm, wv_hbm)):
                copies.append(
                    pltpu.make_async_copy(
                        w_hbm.at[:, pl.ds(h * dim, dim)],
                        w_s.at[h, :, pl.ds(i * dim, dim)],
                        sems.at[base + 2 * h + i],
                    )
                )
        own_copies = copies[base : base + 2 * group]
        other_copies = copies[base + 2 * group :]
        for copy in copies[:base] + own_copies:
            copy.start()

    row = lax.broadcasted_iota(jnp.int32, (CHUNK, CHUNK), 0)
    col = lax.broadcasted_iota(jnp.int32, (CHUNK, CHUNK), 1)
    eye = jnp.where(row == col, 1.0, 0.0)
    upper = jnp.where(row <= col, 1.0, 0.0)

    def level(m):
        return (row // (2 * m) == col // (2 * m)) & (row // m != col // m)

    masks = [jnp.where(level(m), 1.0, 0.0).astype(BF16) for m in steps]
    strict = jnp.where(row > col, 1.0, 0.0).astype(BF16)
    eye_short = eye.astype(BF16)

    if first:
        for copy in copies[:base]:
            copy.wait()
        wd, ws, speeds, ceilings = (ref[...] for ref in small_s[:4])
        mult, spike = (
            jnp.concatenate([ref[s] for s in range(seqs)], axis=1) for ref in small_s[4:]
        )
        table_ref[...] = gate_tables(
            x_s[...].reshape(count, width), wd, ws, speeds, ceilings, mult, spike, heads, upper
        )
        for copy in own_copies:
            copy.wait()
        for copy in other_copies:
            copy.start()
    table = table_ref[...]
    columns = table.T

    def at(c, h, which):
        return (2 * c + which) * heads + h

    def column(c, h, which):
        return jnp.broadcast_to(columns[:, at(c, h, which) : at(c, h, which) + 1], (CHUNK, CHUNK))

    pieces = range(group * chunks)
    lasts, lowers, inverses, fadeds = [], [], [], []

    def prepare(g, raw):
        h = own_heads[g]
        for c in range(chunks):
            n = g * chunks + c
            part = raw[c * CHUNK : (c + 1) * CHUNK].astype(BF16).astype(F32)
            keys = unit(silu(part[:, :dim]))
            values = silu(part[:, dim:])
            strength, total_log = column(c, h, 0), column(c, h, 1)
            last = total_log[CHUNK - 1 : CHUNK]
            short = keys.astype(BF16)
            gram = dot_nt(short, short)
            place = at(c, h, 1)
            spread = jnp.exp(jnp.minimum(total_log - table[place : place + 1], 0.0))
            lower = (gram * strength * spread).astype(BF16) * strict
            lowers.append(lower)
            inverses.append(eye_short - lower * masks[0])
            source_s[n, :, :dim] = keys * (strength * jnp.exp(total_log))
            source_s[n, :, dim:] = values * strength
            fadeds.append((keys * jnp.exp(last - total_log)).astype(BF16))
            lasts.append(jnp.exp(last))

    raws = [
        jnp.concatenate([dot(x_s[s], w_s[h]) for s in range(seqs)], axis=0) for h in own_heads
    ]
    for g in range(group):
        prepare(g, raws[g])

    for i, m in list(enumerate(steps))[1:]:
        if m < 16:
            products = [dot(inverses[n], lowers[n] * masks[i]).astype(BF16) for n in pieces]
            inverses = [
                inverses[n] - dot(products[n], inverses[n]).astype(BF16) for n in pieces
            ]
            continue
        odd = [slice(o, o + m) for o in range(m, CHUNK, 2 * m)]
        products = []
        for n in pieces:
            picked = jnp.concatenate([inverses[n][o] for o in odd], axis=0)
            products.append(dot(picked, lowers[n] * masks[i]).astype(BF16))
        for n in pieces:
            change = dot(products[n], inverses[n]).astype(BF16)
            parts = []
            for j, o in enumerate(odd):
                parts.append(inverses[n][o.start - m : o.start])
                parts.append(inverses[n][o] - change[j * m : (j + 1) * m])
            inverses[n] = jnp.concatenate(parts, axis=0)

    terms = []
    for n in pieces:
        off = inverses[n] - eye_short
        source = source_s[n]
        solved = source + dot(off, source.astype(BF16))
        terms.append(dot_tn(fadeds[n], solved.astype(BF16)))

    per = chunks // seqs
    place = lax.axis_index("sp")
    states = seqs * group
    for g in range(group):
        for s in range(seqs):
            n = g * chunks + s * per
            held_a, held_b = lasts[n] * eye - terms[n][:, :dim], terms[n][:, dim:]
            for n in range(n + 1, n + per):
                change = dot(
                    terms[n][:, :dim].astype(BF16),
                    jnp.concatenate([held_a, held_b], axis=1).astype(BF16),
                )
                held_a = lasts[n] * held_a - change[:, :dim]
                held_b = lasts[n] * held_b - change[:, dim:] + terms[n][:, dim:]
            map_s[s * group + g, :dim, :] = held_a
            map_s[s * group + g, dim:, :] = held_b
    for mask, out in enumerate(outs):
        for i in range(states >> bits):
            out[i] = map_s[state_index(i, place ^ mask, states, bits)]
    if first:
        for copy in other_copies:
            copy.wait()


def local_maps(x, w, small, heads, own_heads, dim, bits, table=None):
    seqs, span, width = x.shape
    count = seqs * span
    group = len(own_heads)
    states = seqs * group
    pieces = group * count // CHUNK
    results = [pltpu.VMEM((states >> bits, 2 * dim, dim), F32)] * 2**bits
    scratch = [
        pltpu.VMEM((pieces, CHUNK, 2 * dim), F32),
        pltpu.VMEM((states, 2 * dim, dim), F32),
    ]
    first = table is None
    if first:
        rows = -(-2 * heads * (count // CHUNK) // PAD) * PAD
        scratch += [pltpu.VMEM(a.shape, a.dtype) for a in small]
        operands = [pltpu.with_memory_space_constraint(a, pltpu.HBM) for a in (x, *w, *small)]
        in_specs = [pl.BlockSpec(memory_space=pltpu.HBM)] * len(operands)
        results = [
            pltpu.VMEM((rows, CHUNK), F32),
            pltpu.VMEM(x.shape, BF16),
            pltpu.VMEM((heads, width, 2 * dim), BF16),
        ] + results
    else:
        operands = [x, w, table]
        in_specs = [WHOLE] * 3
    scratch.append(pltpu.SemaphoreType.DMA((seqs + len(small) + 2 * heads,)))
    return pl.pallas_call(
        lambda *refs: local_maps_kernel(
            *refs, heads=heads, own_heads=own_heads, first=first, bits=bits
        ),
        in_specs=in_specs,
        out_specs=[WHOLE] * len(results),
        out_shape=results,
        scratch_shapes=scratch,
        compiler_params=pltpu.CompilerParams(vmem_limit_bytes=24 * 2**20),
        name="local_maps",
    )(*operands)


def state_index(index, place, states, bits):
    base = index
    for b in range(bits):
        states //= 2
        base = base + ((place >> b) % 2) * states
    return base


def new_token_kernel(
    x_ref, w_ref, wq_ref, wd_ref, ws_ref, speed_ref, ceil_ref, out_ref, *, groups, bits
):
    seqs, _ = x_ref.shape
    dim = w_ref.shape[2] // 2
    heads = w_ref.shape[0]
    states = seqs * len(groups[0]) >> bits
    place = lax.axis_index("sp")
    x = x_ref[...]
    decay_pre = dot_nt(x, wd_ref[...])
    strength_pre = dot_nt(x, ws_ref[...])
    for g, own_heads in enumerate(groups):
        for i in range(states):
            index = state_index(i, place, seqs * len(own_heads), bits)
            s, head = index // len(own_heads), index % len(own_heads) + own_heads[0]
            lane = lax.axis_index("tp") * heads + head
            raw = dot(x, w_ref[head]).astype(BF16).astype(F32)
            lanes = pl.ds(pl.multiple_of(head * dim, dim), dim)
            query_raw = dot(x, wq_ref[:, lanes]).astype(BF16).astype(F32)
            query = unit(silu(query_raw)) * dim ** (-0.5)
            keys = unit(silu(raw[:, :dim]))
            values = silu(raw[:, dim:])
            fading = jnp.exp(
                -pick_lane(speed_ref[:, :heads], head) * softplus(pick_lane(decay_pre, lane))
            )
            match = jnp.sum(query * keys, axis=-1, keepdims=True) * (
                pick_lane(ceil_ref[:, :heads], head) * jax.nn.sigmoid(pick_lane(strength_pre, lane))
            )
            wide = [jnp.broadcast_to(item, query.shape) for item in (fading, match)]
            for n, item in enumerate([query, keys, values, *wide]):
                chosen = item[:1]
                for t in range(1, seqs):
                    chosen = jnp.where(s == t, item[t : t + 1], chosen)
                out_ref[g * states + i, n : n + 1, :] = chosen


def new_token(x, w, wq, small, groups, bits, dim):
    states = x.shape[0] * len(groups[0]) >> bits
    return pl.pallas_call(
        lambda *refs: new_token_kernel(*refs, groups=groups, bits=bits),
        in_specs=[WHOLE] * 7,
        out_specs=WHOLE,
        out_shape=pltpu.VMEM((states * len(groups), PAD, dim), F32),
        compiler_params=LIMIT,
        name="new_token",
    )(x, w, wq, *small[:4])


def compose(early, late, dim):
    early = jnp.concatenate([early[:dim], early[dim:]], axis=1)
    both = dot3(late[:dim], early)
    return jnp.concatenate([both[:, :dim], both[:, dim:] + late[dim:]], axis=0)


def gathered(refs, order_s, i, low, dim):
    place = lax.axis_index("sp") >> low
    count = len(refs)
    for mask, ref in enumerate(refs):
        order_s[(place % count) ^ mask] = ref[i]
    held = [order_s[n] for n in range(count)]
    while len(held) > 1:
        held = [compose(held[n], held[n + 1], dim) for n in range(0, len(held), 2)]
    return held[0]


def merge_kernel(*refs, low):
    ins, out, order_s = refs[:-2], refs[-2], refs[-1]
    for i in range(out.shape[0]):
        out[i] = gathered(ins, order_s, i, low, out.shape[2])


def merge(parts, low):
    shape = parts[0].shape
    return pl.pallas_call(
        lambda *refs: merge_kernel(*refs, low=low),
        in_specs=[WHOLE] * len(parts),
        out_specs=WHOLE,
        out_shape=pltpu.VMEM(shape, F32),
        scratch_shapes=[pltpu.VMEM((len(parts),) + shape[1:], F32)],
        compiler_params=LIMIT,
        name="merge",
    )(*parts)


def pack_kernel(*refs, count, earlier, low, top, last):
    ins, rest = refs[:count], refs[count:]
    befores, rest = rest[:earlier], rest[earlier:]
    if last:
        token_ref, own_ref, send_ref, order_s = rest
    else:
        own_ref, send_ref, full_ref, order_s = rest
    states, _, dim = ins[0].shape
    right = (lax.axis_index("sp") >> top) % 2 == 1
    half = dim // 2
    fulls = []
    for i in range(states):
        full = gathered(ins, order_s, i, low, dim)
        fulls.append(full)
        out_a, out_b = full[:dim], full[dim:]
        at = i * dim
        own_ref[at : at + half, :] = jnp.where(right, out_a[half:], out_b[:half])
        own_ref[at + half : at + dim, :] = out_b[half:]
        send_ref[at : at + half, :] = jnp.where(right, out_a[:half], out_b[:half])
        send_ref[at + half : at + dim, :] = jnp.where(right, out_b[:half], out_b[half:])
        if not last:
            full_ref[i] = full
    if last:
        everything = [ref[i] for ref in befores for i in range(states)] + fulls
        for n, full in enumerate(everything):
            token = token_ref[n]
            reads = dot3(token, jnp.concatenate([full[:dim], full[dim:]], axis=1))
            tail = jnp.concatenate([reads[:2, :dim], reads[:2, dim:]], axis=0)
            at = states * dim + 4 * n
            own_ref[at : at + 4, :] = tail
            send_ref[at : at + 4, :] = tail


def pack(parts, befores, token, low, top):
    states, rows, dim = parts[0].shape
    last = token is not None
    tail = -(-4 * states * (len(befores) + 1) // PAD) * PAD if last else 0
    shape = pltpu.VMEM((states * dim + tail, dim), F32)
    results = [shape, shape] + ([] if last else [pltpu.VMEM(parts[0].shape, F32)])
    operands = [*parts, *befores] + ([token] if last else [])
    return pl.pallas_call(
        lambda *refs: pack_kernel(
            *refs, count=len(parts), earlier=len(befores), low=low, top=top, last=last
        ),
        in_specs=[WHOLE] * len(operands),
        out_specs=[WHOLE] * len(results),
        out_shape=results,
        scratch_shapes=[pltpu.VMEM((len(parts), rows, dim), F32)],
        compiler_params=LIMIT,
        name="pack",
    )(*operands)


def finish_kernel(*refs, count, states, top, block):
    owns, gots = refs[:count], refs[count : 2 * count]
    token_ref, gain_ref = refs[2 * count : 2 * count + 2]
    outs, rows_s = refs[2 * count + 2 : -1], refs[-1]
    dim = gain_ref.shape[1]
    place = lax.axis_index("sp")
    right = (place >> top) % 2 == 1
    half = dim // 2
    reads = []
    total = count * states
    for n in range(total):
        at = n % states * dim
        own, got = owns[n // states][at : at + dim, :], gots[n // states][at : at + dim, :]
        state = jnp.where(right, got, own)
        later = jnp.where(right, own, got)
        at = states * dim + 4 * n
        tail = jnp.where(right, owns[-1][at : at + 4, :], gots[-1][at : at + 4, :])
        full = dot3(jnp.concatenate([later[:half], tail, tail], axis=0), state)
        rows_s[n] = full[:half] + later[half:]
        seen = full[half : half + 2] + tail[2:]
        token = token_ref[n]
        fading, match = token[3:4], token[4:5]
        mixed = fading * (seen[:1] - match * seen[1:2]) + match * token[2:3]
        scale = lax.rsqrt(jnp.mean(mixed * mixed, axis=-1, keepdims=True) + EPS)
        reads.append(mixed * scale * gain_ref[...])
    blocks = half // block
    for mask, out in enumerate(outs):
        start = ((place ^ mask) % blocks) * block
        for n in range(total):
            out[n * block : (n + 1) * block, :] = rows_s[n, pl.ds(start, block), :]
            out[total * block + n : total * block + n + 1, :] = reads[n]


def finish(owns, gots, token, gain, top, bits, block):
    dim = owns[0].shape[1]
    total = token.shape[0]
    states = total // len(owns)
    rows = -(-(total * block + total) // PAD) * PAD
    return pl.pallas_call(
        lambda *refs: finish_kernel(*refs, count=len(owns), states=states, top=top, block=block),
        in_specs=[WHOLE] * (2 * len(owns) + 2),
        out_specs=[WHOLE] * 2**bits,
        out_shape=[pltpu.VMEM((rows, dim), F32)] * 2**bits,
        scratch_shapes=[pltpu.VMEM((total, dim // 2, dim), F32)],
        compiler_params=LIMIT,
        name="finish",
    )(*owns, *gots, token, gain.reshape(1, -1))


def place_kernel(*refs, groups, bits, block):
    count = 2**bits
    ins, cache_ref, read_ref, reads_s = refs[:count], refs[count], refs[count + 1], refs[count + 2]
    seqs, heads, _, dim = cache_ref.shape
    total = seqs * heads // count
    states = total // len(groups)
    place = lax.axis_index("sp")
    for mask, got in enumerate(ins):
        for g, own_heads in enumerate(groups):
            for i in range(states):
                index = state_index(i, place ^ mask, seqs * len(own_heads), bits)
                s, h = index // len(own_heads), index % len(own_heads) + own_heads[0]
                n = g * states + i
                cache_ref[s, h] = got[n * block : (n + 1) * block, :].astype(BF16)
                reads_s[pl.ds(s * heads + h, 1), :] = got[total * block + n : total * block + n + 1, :]
    for h in range(heads):
        rows = [reads_s[s * heads + h : s * heads + h + 1, :] for s in range(seqs)]
        read_ref[:, h * dim : (h + 1) * dim] = jnp.concatenate(rows, axis=0).astype(BF16)


def place_outputs(parts, groups, seqs, heads, dim, block, bits):
    return pl.pallas_call(
        lambda *refs: place_kernel(*refs, groups=groups, bits=bits, block=block),
        in_specs=[WHOLE] * len(parts),
        out_specs=[WHOLE] * 2,
        out_shape=[
            jax.ShapeDtypeStruct((seqs, heads, block, dim), BF16),
            jax.ShapeDtypeStruct((seqs, heads * dim), BF16),
        ],
        scratch_shapes=[pltpu.VMEM((seqs * heads, dim), F32)],
        compiler_params=LIMIT,
        name="place_outputs",
    )(*parts)


def on_device(
    prompt_elements, address_weights, content_weights, lookup_weights, forgetting_weights,
    update_intensity_weights, forgetting_speeds, update_intensity_ceiling, forgetting_multiplier,
    spike_offsets, upcoming_element_vector, retrieval_rms_multiplier,
):
    seqs = prompt_elements.shape[0]
    dim = retrieval_rms_multiplier.shape[0]
    heads = forgetting_speeds.shape[0]
    places = lax.axis_size("sp")
    stages = places.bit_length() - 1
    block = dim // places

    def exchange(values, mask):
        got = lax.ppermute(values, "sp", [(i, i ^ mask) for i in range(places)])
        return pltpu.with_memory_space_constraint(got, pltpu.VMEM)

    parts = 2 if heads % 2 == 0 else 1
    size = heads // parts
    groups = [list(range(g * size, (g + 1) * size)) for g in range(parts)]

    def flat_row(values):
        return jnp.concatenate([values] * (2 if heads == 1 else 1)).reshape(1, -1)

    small = (
        forgetting_weights.T, update_intensity_weights.T, flat_row(forgetting_speeds),
        flat_row(update_intensity_ceiling), forgetting_multiplier.transpose(0, 2, 1),
        spike_offsets.transpose(0, 2, 1),
    )
    bits = min((seqs * size).bit_length() - 1, stages - 1)
    top = stages - 1
    table = None
    flows = []
    x, w = prompt_elements, (address_weights, content_weights)
    for own_heads in groups:
        results = local_maps(x, w, small, heads, own_heads, dim, bits, table)
        if table is None:
            table, x, w, *results = results
        flow = [results[0]] + [None] * (len(results) - 1)
        for m in range(1, len(results)):
            flow[m] = exchange(results[m], m)
        flows.append(flow)
    token = new_token(upcoming_element_vector, w, lookup_weights, small, groups, bits, dim)
    low, span = 0, bits
    while low + span < top:
        for flow in flows:
            joint = merge(flow, low)
            flow[:] = joint, exchange(joint, 2 ** (low + span))
        low, span = low + span, 1
    owns, gots, fulls = [], [], []
    for g, flow in enumerate(flows):
        last = g == len(flows) - 1
        own, send, *full = pack(flow, fulls if last else [], token if last else None, low, top)
        fulls += full
        owns.append(own)
        gots.append(exchange(send, 2**top))
    pieces = finish(owns, gots, token, retrieval_rms_multiplier, top, bits, block)
    pieces = [piece if mask == 0 else exchange(piece, mask) for mask, piece in enumerate(pieces)]
    return tuple(place_outputs(pieces, groups, seqs, heads, dim, block, bits))


def solution(mesh):
    in_specs = (
        P("gr", "sp", None),
        P(None, "tp"),
        P(None, "tp"),
        P(None, "tp"),
        P(),
        P(),
        P("tp"),
        P("tp"),
        P("gr", "sp", "tp"),
        P("gr", "sp", "tp"),
        P("gr", None),
        P(),
    )
    out_specs = (P("gr", "tp", "sp", None), P("gr", "tp"))

    return jax.shard_map(
        on_device, mesh=mesh, in_specs=in_specs, out_specs=out_specs, check_vma=False
    )
```
